32 devices in a mesh: sp: 8 (over z, y), tp: 4 (over x, core).
Axes of the slice: x: 2, y: 2, z: 4, core: 2. Of those that a mesh axis runs over, the one named last changes fastest.
Arguments:
- residual: bfloat16 [2048, 2048], P('sp'), may hold values from -6 to 6
- ssm_input: bfloat16 [2048, 1024], P('sp', 'tp'), may hold values from -6 to 6
- in_map: bfloat16 [2, 64, 16, 128], P(None, 'tp'), may hold values from -1 to 1
- out_map: bfloat16 [2, 64, 16, 128], P(None, 'tp'), may hold values from -0.5 to 0.5
- damping: float32 [64, 64], P('tp'), may hold values from 0.0001 to 0.24
- log_step: float32 [64], P('tp'), may hold values from -8 to -1.2
- frequency: float32 [64, 64], P('tp'), may hold values from 1 to 201.06177
- pacing: float32 [2048], P('sp'), may hold values from 0.28 to 3.5
- feedthrough: float32 [1024], P('tp'), may hold values from -4 to 4
- w_out: bfloat16 [1024, 2048], P('tp'), may hold values from -0.375 to 0.375
- gain_mix: float32 [2048], replicated, may hold values from 0.1 to 1.9
- w_gate: bfloat16 [2048, 5632], P('sp', 'tp'), may hold values from -0.125 to 0.125
- w_value: bfloat16 [2048, 5632], P('sp', 'tp'), may hold values from -0.125 to 0.125
- conv_taps: float32 [3, 5632], P(None, 'tp'), may hold values from -3 to 3
- w_down: bfloat16 [5632, 2048], P('tp', 'sp'), may hold values from -0.21875 to 0.21875
- gain_ffn: float32 [2048], replicated, may hold values from 0.1 to 1.9
Outputs:
- result: bfloat16 [2048, 2048], P(('sp', 'tp'))
The draws below stay inside these ranges and needn't reach their ends.
All inputs are finite; a program needn't handle non-finite values.
Results may differ from the reference program's by a relative error of at most 0.02.
Values may be sent and summed in bfloat16 or wider, within the bound.
A program may use at most 128 MiB of HBM per device.

```python
import math
import jax
import jax.numpy as jnp
from jax import lax

MODEL = 2048
CHANNELS = 1024
GROUP_CH = 16
STATES = 64
FF_UNITS = 5632
GROUPS = 64
LENGTH = 2048
N_TP = 4


def group_law(key):
    keys = jax.random.split(jax.random.fold_in(key, 11), 4)
    fast_share = 0.5
    fast = jax.random.uniform(keys[0], (GROUPS,), jnp.float32) < fast_share
    fast_step = jnp.exp(jax.random.uniform(keys[1], (GROUPS,), jnp.float32, jnp.log(0.2), jnp.log(0.3)))
    slow_rate = jnp.exp(jax.random.uniform(keys[2], (GROUPS,), jnp.float32, jnp.log(0.2), 0.0)) / LENGTH
    slow_step = jnp.sqrt(slow_rate / 0.6)
    step_size = jnp.where(fast, fast_step, slow_step)
    ratio = jax.random.uniform(keys[3], (GROUPS, STATES), jnp.float32, 0.4, 0.8)
    return (step_size, ratio)


def draw_log_step(key, part):
    step_size, ratio = group_law(key)
    return jnp.log(step_size)


def draw_damping(key, part):
    step_size, ratio = group_law(key)
    return step_size[:, None] * ratio


def draw_pacing(key, part):
    keys = jax.random.split(jax.random.fold_in(key, 23), 2)
    spans = LENGTH // 256 + 1
    coarse = jnp.exp(jax.random.uniform(keys[0], (spans,), jnp.float32, jnp.log(0.4), jnp.log(2.5)))
    finer = jnp.exp(jax.random.uniform(keys[1], (LENGTH,), jnp.float32, jnp.log(0.7), jnp.log(1.4)))
    return coarse[jnp.arange(LENGTH) // 256] * finer


def levels(stream_key, shape, pieces, least, high):
    gain = 1.0
    for position, blocks in pieces:
        steps = jax.random.uniform(jax.random.fold_in(jax.random.fold_in(stream_key, 6), position), (blocks,), jnp.float32, least / len(pieces), high / len(pieces))
        gain = gain * jnp.repeat(jnp.exp(steps), shape[position] // blocks).reshape((-1,) + (1,) * (len(shape) - 1 - position))
    return gain


def normal_values(key, dims, scale, most, shards=(), held_as=jnp.bfloat16):
    gain = levels(key, dims, shards, -0.22, 0.18) if shards else 1.0
    drawn = jax.random.normal(key, dims, jnp.float32) * scale * gain
    return jnp.minimum(jnp.maximum(drawn, -most), most).astype(held_as)


def setup_inputs(seed: int = 0) -> dict:
    seeds = jax.random.split(jax.random.key(seed), 17)
    return {
        "residual": normal_values(seeds[0], (LENGTH, MODEL), 1.0, 6.0, ((0, 8),)),
        "ssm_input": normal_values(seeds[1], (LENGTH, CHANNELS), 1.0, 6.0, ((0, 8), (1, 4))),
        "in_map": normal_values(seeds[2], (2, GROUPS, GROUP_CH, 2 * STATES), (2 * GROUP_CH) ** -0.5, 1.0, ((1, 4),)),
        "out_map": normal_values(seeds[3], (2, GROUPS, GROUP_CH, 2 * STATES), (2 * STATES) ** -0.5, 0.5, ((1, 4),)),
        "damping": draw_damping(jax.random.fold_in(seeds[16], 71), 0),
        "log_step": draw_log_step(jax.random.fold_in(seeds[16], 71), 0),
        "frequency": jnp.clip(1.0 + 200.06177 * jax.random.uniform(seeds[6], (GROUPS, STATES), jnp.float32) ** levels(seeds[6], (GROUPS, STATES), ((0, 4),), -0.2, 0.2), 1.0, 201.06177),
        "pacing": draw_pacing(jax.random.fold_in(seeds[16], 71), 0),
        "feedthrough": normal_values(seeds[8], (CHANNELS,), 1.0, 4.0, ((0, 4),), jnp.float32),
        "w_out": normal_values(seeds[9], (CHANNELS, MODEL), (CHANNELS // 4) ** -0.5, 0.375, ((0, 4),)),
        "gain_mix": jnp.clip(1.0 + 0.18 * jax.random.normal(seeds[10], (MODEL,), jnp.float32), 0.1, 1.9),
        "w_gate": normal_values(seeds[11], (MODEL, FF_UNITS), MODEL ** -0.5, 0.125, ((0, 8), (1, 4))),
        "w_value": normal_values(seeds[12], (MODEL, FF_UNITS), MODEL ** -0.5, 0.125, ((0, 8), (1, 4))),
        "conv_taps": normal_values(seeds[13], (3, FF_UNITS), 0.577, 3.0, ((1, 4),), jnp.float32),
        "w_down": normal_values(seeds[14], (FF_UNITS, MODEL), (FF_UNITS // 8) ** -0.5, 0.21875, ((0, 4), (1, 8))),
        "gain_ffn": jnp.clip(1.0 + 0.18 * jax.random.normal(seeds[15], (MODEL,), jnp.float32), 0.1, 1.9),
    }


deep_alpha = 8.0 ** 0.25
norm_eps = 1e-06
highest = lax.Precision.HIGHEST

def normalize(pre_norm, gain_row):
    mean_row = lax.optimization_barrier(jnp.mean(pre_norm, axis=-1, keepdims=True))
    centred = pre_norm - mean_row
    spread = lax.optimization_barrier(jnp.mean(centred * centred, axis=-1, keepdims=True))
    return centred * lax.rsqrt(spread + norm_eps) * gain_row

def complex_mul(a_re, a_im, b_re, b_im):
    return (a_re * b_re - a_im * b_im, a_re * b_im + a_im * b_re)

def one_direction(u_groups, pacing, in_map_d, out_map_d, damping, frequency, step_size, backward):
    length = u_groups.shape[0]
    groups = u_groups.shape[1]
    group_width = u_groups.shape[2]
    state_half = damping.shape[1]
    block_len = math.gcd(length, 512)
    blocks = length // block_len
    rate_re = -damping
    rate_im = frequency
    modulus = rate_re * rate_re + rate_im * rate_im
    in_full = in_map_d.astype(jnp.float32)
    out_full = out_map_d.astype(jnp.float32)

    def per_block(state_pair, inputs_now):
        u_block, pace_block = inputs_now
        inflow = jnp.einsum('tgc,gcq->tgq', u_block, in_full, precision=highest)
        deltas = step_size[None, :, None] * pace_block[:, None, None]
        magnitude = jnp.exp(rate_re[None] * deltas)
        decay_re = magnitude * jnp.cos(rate_im[None] * deltas)
        decay_im = magnitude * jnp.sin(rate_im[None] * deltas)
        less_one = decay_re - 1.0
        factor_re = (less_one * rate_re + decay_im * rate_im) / modulus
        factor_im = (decay_im * rate_re - less_one * rate_im) / modulus
        drive_re, drive_im = complex_mul(factor_re, factor_im, inflow[..., :state_half], inflow[..., state_half:])

        def advance(carry_pair, step_terms):
            old_re, old_im = carry_pair
            dec_re, dec_im, add_re, add_im = step_terms
            new_re, new_im = complex_mul(dec_re, dec_im, old_re, old_im)
            new_re = new_re + add_re
            new_im = new_im + add_im
            return ((new_re, new_im), jnp.concatenate([new_re, new_im], axis=-1))
        state_pair, sequence = lax.scan(advance, state_pair, (decay_re, decay_im, drive_re, drive_im), reverse=backward)
        readout = jnp.einsum('tgq,gcq->tgc', sequence, out_full, precision=highest)
        return (state_pair, readout)
    empty_state = jnp.zeros((groups, state_half), jnp.float32)
    u_blocks = u_groups.reshape(blocks, block_len, groups, group_width)
    pace_blocks = pacing.reshape(blocks, block_len)
    final_pair, readouts = lax.scan(per_block, (empty_state, empty_state), (u_blocks, pace_blocks), reverse=backward)
    return readouts.reshape(length, groups, group_width)

def blockwise(rows_in, weights):
    block_width = rows_in.shape[1] // N_TP
    running = jnp.zeros((rows_in.shape[0], weights.shape[1]), jnp.float32)
    for block_index in range(N_TP):
        first_col = block_index * block_width
        partial_value = jnp.dot(rows_in[:, first_col:first_col + block_width], weights[first_col:first_col + block_width], preferred_element_type=jnp.float32)
        running = running + lax.optimization_barrier(partial_value.astype(jnp.bfloat16)).astype(jnp.float32)
    return running

def reference(residual, ssm_input, in_map, out_map, damping, log_step, frequency, pacing, feedthrough, w_out, gain_mix, w_gate, w_value, conv_taps, w_down, gain_ffn):
    length = ssm_input.shape[0]
    channel_count = ssm_input.shape[1]
    groups = damping.shape[0]
    group_width = channel_count // groups
    step_size = jnp.exp(log_step)
    inputs_f = ssm_input.astype(jnp.float32)
    u_groups = inputs_f.reshape(length, groups, group_width)
    readout = one_direction(u_groups, pacing, in_map[0], out_map[0], damping, frequency, step_size, False)
    readout = readout + one_direction(u_groups, pacing, in_map[1], out_map[1], damping, frequency, step_size, True)
    readout = readout.reshape(length, channel_count) + feedthrough * inputs_f
    channels = jax.nn.gelu(readout).astype(jnp.bfloat16)
    mixed = blockwise(channels, w_out)
    norm_first = normalize(deep_alpha * residual.astype(jnp.float32) + mixed, gain_mix)
    norm_first = lax.optimization_barrier(norm_first.astype(jnp.bfloat16))
    ff_block = w_gate.shape[1] // N_TP
    branch = jnp.zeros(residual.shape, jnp.float32)
    for block_index in range(N_TP):
        first_col = block_index * ff_block
        gated = jnp.dot(norm_first, w_gate[:, first_col:first_col + ff_block], preferred_element_type=jnp.float32)
        gated = lax.optimization_barrier(gated.astype(jnp.bfloat16))
        values = jnp.dot(norm_first, w_value[:, first_col:first_col + ff_block], preferred_element_type=jnp.float32)
        values = lax.optimization_barrier(values.astype(jnp.bfloat16))
        padded = jnp.pad(gated.astype(jnp.float32), ((1, 1), (0, 0)))
        taps_now = conv_taps[:, first_col:first_col + ff_block]
        smoothed = taps_now[0] * padded[:-2] + taps_now[1] * padded[1:-1] + taps_now[2] * padded[2:]
        hidden = (jax.nn.gelu(smoothed) * values.astype(jnp.float32)).astype(jnp.bfloat16)
        partial_value = jnp.dot(hidden, w_down[first_col:first_col + ff_block], preferred_element_type=jnp.float32)
        branch = branch + lax.optimization_barrier(partial_value.astype(jnp.bfloat16)).astype(jnp.float32)
    result = normalize(deep_alpha * norm_first.astype(jnp.float32) + branch, gain_ffn)
    return result.astype(jnp.bfloat16)
```

```python
import functools
import math

import jax
import jax.numpy as jnp
from jax import lax
from jax.experimental import pallas as pl
from jax.experimental.pallas import tpu as pltpu
from jax.sharding import PartitionSpec as P

deep_alpha = 8.0**0.25
norm_eps = 1e-06
LANES = 128
SUB = 8
MESH = pl.DeviceIdType.MESH
F32 = jnp.float32
BF16 = jnp.bfloat16


def cmul(ar, ai, br, bi):
    return ar * br - ai * bi, ar * bi + ai * br


def sincos(angle):
    turns = jnp.floor(angle * (1.0 / (2.0 * math.pi)) + 0.5)
    rest = (angle - turns * 6.28125) - turns * (2.0 * math.pi - 6.28125)
    half = 0.5 * rest
    sq = half * half
    s = -1.0 / 39916800.0
    for c in (1.0 / 362880.0, -1.0 / 5040.0, 1.0 / 120.0, -1.0 / 6.0, 1.0):
        s = s * sq + c
    s = s * half
    c0 = 1.0 / 479001600.0
    for c in (-1.0 / 3628800.0, 1.0 / 40320.0, -1.0 / 720.0, 1.0 / 24.0, -0.5, 1.0):
        c0 = c0 * sq + c
    return 2.0 * s * c0, 1.0 - 2.0 * s * s


def normalize(pre, gain):
    mean = jnp.mean(pre, axis=-1, keepdims=True)
    cen = pre - mean
    spread = jnp.mean(cen * cen, axis=-1, keepdims=True)
    return cen * lax.rsqrt(spread + norm_eps) * gain


def gelu(x):
    return 0.5 * x * (1.0 + jnp.tanh(0.7978845608028654 * (x + 0.044715 * (x * x * x))))


def tile_ds(tile):
    return pl.ds(pl.multiple_of(tile * LANES, LANES), LANES)


def scan_kernel(half, width, u_ref, pace_ref, rows_ref, in_ref, sf_ref, sb_ref, pf_ref, pb_ref, tot_ref, flow, dec):
    positions = u_ref.shape[0]
    steps = positions // SUB
    tiles = rows_ref.shape[1] // LANES
    per_tile = LANES // half
    chans = u_ref.shape[1]
    row_group = lax.broadcasted_iota(jnp.int32, (chans, LANES), 0) // width
    lane_group = lax.broadcasted_iota(jnp.int32, (chans, LANES), 1) // half

    @pl.loop(0, tiles)
    def _(tile):
        lanes = tile_ds(tile)
        mask = row_group == lane_group + tile * per_tile
        for k in range(4):
            w = jnp.where(mask, in_ref[k].astype(F32), 0.0).astype(BF16)
            flow[k] = jnp.dot(u_ref[...], w, preferred_element_type=F32)
        step = rows_ref[0:1, lanes]
        damp = rows_ref[1:2, lanes]
        freq = rows_ref[2:3, lanes]
        ir = rows_ref[3:4, lanes]
        ii = rows_ref[4:5, lanes]
        one = jnp.ones((SUB, LANES), F32)
        zero = jnp.zeros((SUB, LANES), F32)

        def ahead(j, carry):
            sr, si, pr, pi = carry
            at = pl.ds(pl.multiple_of(j * SUB, SUB), SUB)
            delta = step * pace_ref[at, :]
            mag = jnp.exp(damp * delta)
            sn, cs = sincos(freq * delta)
            dr, di = mag * cs, mag * sn
            fr, fi = cmul(dr - 1.0, di, ir, ii)
            vr, vi = cmul(fr, fi, flow[0, at, :], flow[1, at, :])
            br, bi = cmul(fr, fi, flow[2, at, :], flow[3, at, :])
            flow[2, at, :] = br
            flow[3, at, :] = bi
            dec[0, at, :] = dr
            dec[1, at, :] = di
            sr, si = cmul(dr, di, sr, si)
            sr, si = sr + vr, si + vi
            pr, pi = cmul(dr, di, pr, pi)
            sf_ref[0, at, lanes] = sr
            sf_ref[1, at, lanes] = si
            pf_ref[0, at, lanes] = pr
            pf_ref[1, at, lanes] = pi
            return sr, si, pr, pi

        efr, efi, tr, ti = lax.fori_loop(0, steps, ahead, (zero, zero, one, zero), unroll=4)

        def behind(k, carry):
            sr, si, pr, pi = carry
            at = pl.ds(pl.multiple_of((steps - 1 - k) * SUB, SUB), SUB)
            dr, di = dec[0, at, :], dec[1, at, :]
            sr, si = cmul(dr, di, sr, si)
            sr, si = sr + flow[2, at, :], si + flow[3, at, :]
            pr, pi = cmul(dr, di, pr, pi)
            sb_ref[0, at, lanes] = sr
            sb_ref[1, at, lanes] = si
            pb_ref[0, at, lanes] = pr
            pb_ref[1, at, lanes] = pi
            return sr, si, pr, pi

        ebr, ebi, _, _ = lax.fori_loop(0, steps, behind, (zero, zero, one, zero), unroll=4)
        for k, v in enumerate((efr, efi, ebr, ebi, tr, ti)):
            tot_ref[k, :, lanes] = v


def join_chunks(tot, backward):
    n = tot.shape[1]
    off = 2 if backward else 0
    order = range(n - 1, -1, -1) if backward else range(n)
    cr = jnp.zeros_like(tot[0, 0])
    ci = jnp.zeros_like(cr)
    starts = [None] * n
    for s in order:
        starts[s] = (cr, ci)
        nr, ni = cmul(tot[4, s], tot[5, s], cr, ci)
        cr, ci = nr + tot[off, s], ni + tot[off + 1, s]
    return jnp.stack([a for a, _ in starts]), jnp.stack([b for _, b in starts]), cr, ci


def share_kernel(axis, n, x_ref, out_ref, got, send, recv):
    me = lax.axis_index(axis)
    barrier = pltpu.get_barrier_semaphore()
    for k in range(1, n):
        pl.semaphore_signal(barrier, inc=1, device_id={axis: lax.rem(me + k, n)}, device_id_type=MESH)
    pl.semaphore_wait(barrier, n - 1)
    copies = []
    for k in range(1, n):
        c = pltpu.make_async_remote_copy(
            src_ref=x_ref, dst_ref=got.at[k - 1], send_sem=send.at[k - 1], recv_sem=recv.at[k - 1],
            device_id={axis: lax.rem(me + k, n)}, device_id_type=MESH)
        c.start()
        copies.append(c)
    for c in copies:
        c.wait()
    out_ref[...] = got[...]


def share(x, axis, cid):
    n = lax.axis_size(axis)
    return pl.pallas_call(
        functools.partial(share_kernel, axis, n),
        out_shape=jax.ShapeDtypeStruct((n - 1,) + x.shape, x.dtype),
        in_specs=[pl.BlockSpec(memory_space=pltpu.VMEM)],
        out_specs=pl.BlockSpec(memory_space=pltpu.VMEM),
        scratch_shapes=[pltpu.VMEM((n - 1,) + x.shape, x.dtype),
                        pltpu.SemaphoreType.DMA((n - 1,)), pltpu.SemaphoreType.DMA((n - 1,))],
        compiler_params=pltpu.CompilerParams(collective_id=cid, has_side_effects=True),
        name="share_ends",
    )(x)


def readout_kernel(half, width, sf_ref, sb_ref, pf_ref, pb_ref, cin_ref, out_ref, u_ref, feed_ref, wo_ref, mixed_ref, acc):
    positions = u_ref.shape[0]
    steps = positions // SUB
    tiles = cin_ref.shape[2] // LANES
    per_tile = LANES // half
    chans = u_ref.shape[1]
    col_group = lax.broadcasted_iota(jnp.int32, (LANES, chans), 1) // width
    row_group = lax.broadcasted_iota(jnp.int32, (LANES, chans), 0) // half
    acc[...] = feed_ref[...] * u_ref[...].astype(F32)

    @pl.loop(0, tiles)
    def _(tile):
        lanes = tile_ds(tile)
        mask = col_group == row_group + tile * per_tile
        total = acc[...]
        for d, (s_ref, p_ref) in enumerate(((sf_ref, pf_ref), (sb_ref, pb_ref))):
            cr = jnp.broadcast_to(cin_ref[2 * d, :, lanes][None], (steps, SUB, LANES)).reshape(positions, LANES)
            ci = jnp.broadcast_to(cin_ref[2 * d + 1, :, lanes][None], (steps, SUB, LANES)).reshape(positions, LANES)
            ar, ai = cmul(p_ref[0, :, lanes], p_ref[1, :, lanes], cr, ci)
            for k, st in enumerate((ar + s_ref[0, :, lanes], ai + s_ref[1, :, lanes])):
                w = jnp.where(mask, out_ref[2 * d + k].astype(F32), 0.0).astype(BF16)
                total += jnp.dot(st.astype(BF16), w, preferred_element_type=F32)
        acc[...] = total

    channels = gelu(acc[...]).astype(BF16)
    row = lax.broadcasted_iota(jnp.int32, (positions, positions), 0)
    col = lax.broadcasted_iota(jnp.int32, (positions, positions), 1)
    pick = jnp.where(col == lax.rem(row, steps) * SUB + row // steps, 1.0, 0.0).astype(BF16)
    channels = jnp.dot(pick, channels, preferred_element_type=F32).astype(BF16)
    cols = wo_ref.shape[1]
    piece = min(512, cols)
    for c in range(cols // piece):
        at = slice(c * piece, (c + 1) * piece)
        mixed_ref[:, at] = jnp.dot(channels, wo_ref[:, at], preferred_element_type=F32).astype(BF16)


def settle_kernel(axis, n, spread, part_ref, res_ref, gain_ref, out_ref, got, whole, s1, r1, s2, r2):
    me = lax.axis_index(axis)
    rows = part_ref.shape[0] // n
    barrier = pltpu.get_barrier_semaphore()
    for k in range(1, n):
        pl.semaphore_signal(barrier, inc=1, device_id={axis: lax.rem(me + k, n)}, device_id_type=MESH)
    pl.semaphore_wait(barrier, n - 1)

    def span(who):
        return pl.ds(pl.multiple_of(who * rows, rows), rows)

    copies = []
    for k in range(1, n):
        peer = lax.rem(me + k, n)
        c = pltpu.make_async_remote_copy(
            src_ref=part_ref.at[span(peer)], dst_ref=got.at[k - 1], send_sem=s1.at[k - 1],
            recv_sem=r1.at[k - 1], device_id={axis: peer}, device_id_type=MESH)
        c.start()
        copies.append(c)
    total = part_ref[span(me), :].astype(F32)
    own = res_ref[span(me), :] if spread else res_ref[...]
    total = total + deep_alpha * own.astype(F32)
    for k in range(1, n):
        copies[k - 1].wait()
        total = total + got[k - 1].astype(F32)
    result = normalize(total, gain_ref[...]).astype(BF16)
    if not spread:
        out_ref[...] = result
        return
    whole[0] = result
    copies = []
    for k in range(1, n):
        c = pltpu.make_async_remote_copy(
            src_ref=whole.at[0], dst_ref=whole.at[k], send_sem=s2.at[k - 1], recv_sem=r2.at[k - 1],
            device_id={axis: lax.rem(me + k, n)}, device_id_type=MESH)
        c.start()
        copies.append(c)
    out_ref[span(me), :] = result
    for k in range(1, n):
        copies[k - 1].wait()
        out_ref[span(lax.rem(me + n - k, n)), :] = whole[k]


def settle(part, res, gain, axis, spread, cid):
    n = lax.axis_size(axis)
    rows = part.shape[0] // n
    width = part.shape[1]
    dma = pltpu.SemaphoreType.DMA((n - 1,))
    return pl.pallas_call(
        functools.partial(settle_kernel, axis, n, spread),
        out_shape=jax.ShapeDtypeStruct((part.shape[0] if spread else rows, width), BF16),
        in_specs=[pl.BlockSpec(memory_space=pltpu.VMEM)] * 3,
        out_specs=pl.BlockSpec(memory_space=pltpu.VMEM),
        scratch_shapes=[pltpu.VMEM((n - 1, rows, width), BF16), pltpu.VMEM((n, rows, width), BF16),
                        dma, dma, dma, dma],
        compiler_params=pltpu.CompilerParams(collective_id=cid, has_side_effects=True),
        cost_estimate=pl.CostEstimate(flops=2 * 10**9, bytes_accessed=part.size * 4, transcendentals=0),
        name="settle_spread" if spread else "settle_last",
    )(part, res, gain.reshape(1, -1))


def vmem(count):
    return [pl.BlockSpec(memory_space=pltpu.VMEM)] * count


def state_space(ssm_input, in_map, out_map, damping, log_step, frequency, pacing, feedthrough, w_out):
    positions, chans = ssm_input.shape
    groups, half = damping.shape
    width = chans // groups
    steps = positions // SUB
    flat = groups * half
    step = jnp.exp(log_step)[:, None] * jnp.ones((1, half), F32)
    modulus = damping * damping + frequency * frequency
    rows = jnp.stack([step, -damping, frequency, -damping / modulus, -frequency / modulus]).reshape(5, flat)
    u = ssm_input.reshape(SUB, steps, chans).transpose(1, 0, 2).reshape(positions, chans)
    pace = pacing.reshape(SUB, steps).T.reshape(positions, 1) * jnp.ones((1, LANES), F32)
    reps = LANES // half
    in_cols = in_map.reshape(2, chans, 2, half).transpose(0, 2, 1, 3).reshape(4, chans, half)
    in_cols = jnp.tile(in_cols, (1, 1, reps))
    out_rows = out_map.reshape(2, chans, 2, half).transpose(0, 2, 3, 1).reshape(4, half, chans)
    out_rows = jnp.tile(out_rows, (1, reps, 1))
    big = jax.ShapeDtypeStruct((2, positions, flat), F32)
    sf, sb, pf, pb, tot = pl.pallas_call(
        functools.partial(scan_kernel, half, width),
        out_shape=(big, big, big, big, jax.ShapeDtypeStruct((6, SUB, flat), F32)),
        in_specs=vmem(4),
        out_specs=tuple(vmem(5)),
        scratch_shapes=[pltpu.VMEM((4, positions, LANES), F32), pltpu.VMEM((2, positions, LANES), F32)],
        cost_estimate=pl.CostEstimate(flops=4 * 10**9, bytes_accessed=10**7, transcendentals=0),
        name="scan_local",
    )(u, pace, rows, in_cols)
    fr, fi, fer, fei = join_chunks(tot, False)
    br, bi, ber, bei = join_chunks(tot, True)
    ones, zeros = jnp.ones((flat,), F32), jnp.zeros((flat,), F32)
    pre = [(ones, zeros)]
    suf = [(ones, zeros)]
    for s in range(SUB):
        pre.append(cmul(*pre[-1], tot[4, s], tot[5, s]))
        suf.append(cmul(*suf[-1], tot[4, SUB - 1 - s], tot[5, SUB - 1 - s]))
    mine = jnp.stack([fer, fei, ber, bei, pre[-1][0], pre[-1][1]]).reshape(6, flat // LANES, LANES)
    n = lax.axis_size("sp")
    me = lax.axis_index("sp")
    got = share(mine, "sp", 3).reshape(n - 1, 6, flat)
    cfr, cfi, cbr, cbi = zeros, zeros, zeros, zeros
    for k in range(n - 1, 0, -1):
        far = got[k - 1]
        nr, ni = cmul(far[4], far[5], cfr, cfi)
        use = me - k >= 0
        cfr, cfi = jnp.where(use, nr + far[0], cfr), jnp.where(use, ni + far[1], cfi)
        far = got[n - k - 1]
        nr, ni = cmul(far[4], far[5], cbr, cbi)
        use = me + k < n
        cbr, cbi = jnp.where(use, nr + far[2], cbr), jnp.where(use, ni + far[3], cbi)
    prr = jnp.stack([p[0] for p in pre[:-1]])
    pri = jnp.stack([p[1] for p in pre[:-1]])
    sur = jnp.stack([p[0] for p in suf[:-1]][::-1])
    sui = jnp.stack([p[1] for p in suf[:-1]][::-1])
    ar, ai = cmul(prr, pri, cfr, cfi)
    er, ei = cmul(sur, sui, cbr, cbi)
    cin = jnp.stack([fr + ar, fi + ai, br + er, bi + ei])
    return pl.pallas_call(
        functools.partial(readout_kernel, half, width),
        out_shape=jax.ShapeDtypeStruct((positions, w_out.shape[1]), BF16),
        in_specs=vmem(9),
        out_specs=pl.BlockSpec(memory_space=pltpu.VMEM),
        scratch_shapes=[pltpu.VMEM((positions, chans), F32)],
        cost_estimate=pl.CostEstimate(flops=4 * 10**9, bytes_accessed=10**7, transcendentals=0),
        name="read_states",
    )(sf, sb, pf, pb, cin, out_rows, u, feedthrough.reshape(1, -1), w_out)


def edges(gated):
    n = lax.axis_size("sp")
    before = lax.ppermute(gated[-1:], "sp", [(i, i + 1) for i in range(n - 1)])
    after = lax.ppermute(gated[:1], "sp", [(i + 1, i) for i in range(n - 1)])
    return jnp.concatenate([before, gated, after], axis=0)


def shards(residual, ssm_input, in_map, out_map, damping, log_step, frequency, pacing, feedthrough,
           w_out, gain_mix, w_gate, w_value, conv_taps, w_down, gain_ffn):
    positions = ssm_input.shape[0]
    own_rows = positions // lax.axis_size("tp")
    gate_all = lax.all_gather(w_gate, "sp", axis=0, tiled=True)
    value_all = lax.all_gather(w_value, "sp", axis=0, tiled=True)
    down_all = lax.all_gather(w_down, "sp", axis=1, tiled=True)
    partial = state_space(ssm_input, in_map, out_map, damping, log_step, frequency, pacing, feedthrough, w_out)
    rows = settle(partial, residual, gain_mix, "tp", True, 4)
    gated = jnp.dot(rows, gate_all, preferred_element_type=F32).astype(BF16)
    padded = edges(gated).astype(F32)
    values = jnp.dot(rows, value_all, preferred_element_type=F32).astype(BF16).astype(F32)
    smoothed = conv_taps[0] * padded[:-2] + conv_taps[1] * padded[1:-1] + conv_taps[2] * padded[2:]
    hidden = (jax.nn.gelu(smoothed) * values).astype(BF16)
    parts = jnp.dot(hidden, down_all, preferred_element_type=F32).astype(BF16)
    kept = lax.dynamic_slice_in_dim(rows, lax.axis_index("tp") * own_rows, own_rows, 0)
    return settle(parts, kept, gain_ffn, "tp", False, 5)


def solution(mesh):
    in_specs = (
        P("sp", None), P("sp", "tp"), P(None, "tp", None, None), P(None, "tp", None, None),
        P("tp", None), P("tp"), P("tp", None), P("sp"), P("tp"), P("tp", None), P(),
        P("sp", "tp"), P("sp", "tp"), P(None, "tp"), P("tp", "sp"), P(),
    )
    return jax.shard_map(shards, mesh=mesh, in_specs=in_specs, out_specs=P(("sp", "tp"), None), check_vma=False)
```

```python
import functools
import math

import jax
import jax.numpy as jnp
from jax import lax
from jax.experimental import pallas as pl
from jax.experimental.pallas import tpu as pltpu
from jax.sharding import PartitionSpec as P

deep_alpha = 8.0**0.25
norm_eps = 1e-06
LANES = 128
SUB = 8
MESH = pl.DeviceIdType.MESH
F32 = jnp.float32
BF16 = jnp.bfloat16


def cmul(ar, ai, br, bi):
    return ar * br - ai * bi, ar * bi + ai * br


def sincos(angle):
    turns = jnp.floor(angle * (1.0 / (2.0 * math.pi)) + 0.5)
    rest = (angle - turns * 6.28125) - turns * (2.0 * math.pi - 6.28125)
    half = 0.5 * rest
    sq = half * half
    s = -1.0 / 39916800.0
    for c in (1.0 / 362880.0, -1.0 / 5040.0, 1.0 / 120.0, -1.0 / 6.0, 1.0):
        s = s * sq + c
    s = s * half
    c0 = 1.0 / 479001600.0
    for c in (-1.0 / 3628800.0, 1.0 / 40320.0, -1.0 / 720.0, 1.0 / 24.0, -0.5, 1.0):
        c0 = c0 * sq + c
    return 2.0 * s * c0, 1.0 - 2.0 * s * s


def normalize(pre, gain):
    mean = jnp.mean(pre, axis=-1, keepdims=True)
    cen = pre - mean
    spread = jnp.mean(cen * cen, axis=-1, keepdims=True)
    return cen * lax.rsqrt(spread + norm_eps) * gain


def gelu(x):
    return 0.5 * x * (1.0 + jnp.tanh(0.7978845608028654 * (x + 0.044715 * (x * x * x))))


def tile_ds(tile):
    return pl.ds(pl.multiple_of(tile * LANES, LANES), LANES)


def scan_kernel(half, width, u_ref, pace_ref, rows_ref, in_ref, sf_ref, sb_ref, pf_ref, pb_ref, tot_ref, flow, dec):
    positions = u_ref.shape[0]
    steps = positions // SUB
    tiles = rows_ref.shape[1] // LANES
    per_tile = LANES // half
    chans = u_ref.shape[1]
    row_group = lax.broadcasted_iota(jnp.int32, (chans, LANES), 0) // width
    lane_group = lax.broadcasted_iota(jnp.int32, (chans, LANES), 1) // half

    @pl.loop(0, tiles)
    def _(tile):
        lanes = tile_ds(tile)
        mask = row_group == lane_group + tile * per_tile
        for k in range(4):
            w = jnp.where(mask, in_ref[k].astype(F32), 0.0).astype(BF16)
            flow[k] = jnp.dot(u_ref[...], w, preferred_element_type=F32)
        step = rows_ref[0:1, lanes]
        damp = rows_ref[1:2, lanes]
        freq = rows_ref[2:3, lanes]
        ir = rows_ref[3:4, lanes]
        ii = rows_ref[4:5, lanes]
        one = jnp.ones((SUB, LANES), F32)
        zero = jnp.zeros((SUB, LANES), F32)

        def ahead(j, carry):
            sr, si, pr, pi = carry
            at = pl.ds(pl.multiple_of(j * SUB, SUB), SUB)
            delta = step * pace_ref[at, :]
            mag = jnp.exp(damp * delta)
            sn, cs = sincos(freq * delta)
            dr, di = mag * cs, mag * sn
            fr, fi = cmul(dr - 1.0, di, ir, ii)
            vr, vi = cmul(fr, fi, flow[0, at, :], flow[1, at, :])
            br, bi = cmul(fr, fi, flow[2, at, :], flow[3, at, :])
            flow[2, at, :] = br
            flow[3, at, :] = bi
            dec[0, at, :] = dr
            dec[1, at, :] = di
            sr, si = cmul(dr, di, sr, si)
            sr, si = sr + vr, si + vi
            pr, pi = cmul(dr, di, pr, pi)
            sf_ref[0, at, lanes] = sr
            sf_ref[1, at, lanes] = si
            pf_ref[0, at, lanes] = pr
            pf_ref[1, at, lanes] = pi
            return sr, si, pr, pi

        efr, efi, tr, ti = lax.fori_loop(0, steps, ahead, (zero, zero, one, zero), unroll=4)

        def behind(k, carry):
            sr, si, pr, pi = carry
            at = pl.ds(pl.multiple_of((steps - 1 - k) * SUB, SUB), SUB)
            dr, di = dec[0, at, :], dec[1, at, :]
            sr, si = cmul(dr, di, sr, si)
            sr, si = sr + flow[2, at, :], si + flow[3, at, :]
            pr, pi = cmul(dr, di, pr, pi)
            sb_ref[0, at, lanes] = sr
            sb_ref[1, at, lanes] = si
            pb_ref[0, at, lanes] = pr
            pb_ref[1, at, lanes] = pi
            return sr, si, pr, pi

        ebr, ebi, _, _ = lax.fori_loop(0, steps, behind, (zero, zero, one, zero), unroll=4)
        for k, v in enumerate((efr, efi, ebr, ebi, tr, ti)):
            tot_ref[k, :, lanes] = v


def readout_kernel(half, width, sf_ref, sb_ref, pf_ref, pb_ref, cin_ref, out_ref, u_ref, feed_ref, wo_ref, mixed_ref, acc):
    positions = u_ref.shape[0]
    steps = positions // SUB
    tiles = cin_ref.shape[2] // LANES
    per_tile = LANES // half
    chans = u_ref.shape[1]
    col_group = lax.broadcasted_iota(jnp.int32, (LANES, chans), 1) // width
    row_group = lax.broadcasted_iota(jnp.int32, (LANES, chans), 0) // half
    acc[...] = feed_ref[...] * u_ref[...].astype(F32)

    @pl.loop(0, tiles)
    def _(tile):
        lanes = tile_ds(tile)
        mask = col_group == row_group + tile * per_tile
        total = acc[...]
        for d, (s_ref, p_ref) in enumerate(((sf_ref, pf_ref), (sb_ref, pb_ref))):
            cr = jnp.broadcast_to(cin_ref[2 * d, :, lanes][None], (steps, SUB, LANES)).reshape(positions, LANES)
            ci = jnp.broadcast_to(cin_ref[2 * d + 1, :, lanes][None], (steps, SUB, LANES)).reshape(positions, LANES)
            ar, ai = cmul(p_ref[0, :, lanes], p_ref[1, :, lanes], cr, ci)
            for k, st in enumerate((ar + s_ref[0, :, lanes], ai + s_ref[1, :, lanes])):
                w = jnp.where(mask, out_ref[2 * d + k].astype(F32), 0.0).astype(BF16)
                total += jnp.dot(st.astype(BF16), w, preferred_element_type=F32)
        acc[...] = total

    channels = gelu(acc[...]).astype(BF16)
    row = lax.broadcasted_iota(jnp.int32, (positions, positions), 0)
    col = lax.broadcasted_iota(jnp.int32, (positions, positions), 1)
    pick = jnp.where(col == lax.rem(row, steps) * SUB + row // steps, 1.0, 0.0).astype(BF16)
    channels = jnp.dot(pick, channels, preferred_element_type=F32).astype(BF16)
    cols = wo_ref.shape[1]
    piece = min(512, cols)
    for c in range(cols // piece):
        at = slice(c * piece, (c + 1) * piece)
        mixed_ref[:, at] = jnp.dot(channels, wo_ref[:, at], preferred_element_type=F32).astype(BF16)


def settle_kernel(axis, n, spread, part_ref, *refs):
    me = lax.axis_index(axis)
    barrier = pltpu.get_barrier_semaphore()
    for k in range(1, n):
        pl.semaphore_signal(barrier, inc=1, device_id={axis: lax.rem(me + k, n)}, device_id_type=MESH)
    pl.semaphore_wait(barrier, n - 1)
    settle_body(axis, n, spread, part_ref, *refs)


def settle_body(axis, n, spread, part_ref, res_ref, gain_ref, out_ref, got, whole, s1, r1, s2, r2):
    me = lax.axis_index(axis)
    rows = part_ref.shape[0] // n

    def span(who):
        return pl.ds(pl.multiple_of(who * rows, rows), rows)

    copies = []
    for k in range(1, n):
        peer = lax.rem(me + k, n)
        c = pltpu.make_async_remote_copy(
            src_ref=part_ref.at[span(peer)], dst_ref=got.at[k - 1], send_sem=s1.at[k - 1],
            recv_sem=r1.at[k - 1], device_id={axis: peer}, device_id_type=MESH)
        c.start()
        copies.append(c)
    total = part_ref[span(me), :].astype(F32)
    own = res_ref[span(me), :] if spread else res_ref[...]
    total = total + deep_alpha * own.astype(F32)
    for k in range(1, n):
        copies[k - 1].wait()
        total = total + got[k - 1].astype(F32)
    result = normalize(total, gain_ref[...]).astype(BF16)
    if not spread:
        out_ref[...] = result
        return
    whole[0] = result
    copies = []
    for k in range(1, n):
        c = pltpu.make_async_remote_copy(
            src_ref=whole.at[0], dst_ref=whole.at[k], send_sem=s2.at[k - 1], recv_sem=r2.at[k - 1],
            device_id={axis: lax.rem(me + k, n)}, device_id_type=MESH)
        c.start()
        copies.append(c)
    out_ref[span(me), :] = result
    for k in range(1, n):
        copies[k - 1].wait()
        out_ref[span(lax.rem(me + n - k, n)), :] = whole[k]


def settle(part, res, gain, axis, spread, cid):
    n = lax.axis_size(axis)
    rows = part.shape[0] // n
    width = part.shape[1]
    dma = pltpu.SemaphoreType.DMA((n - 1,))
    return pl.pallas_call(
        functools.partial(settle_kernel, axis, n, spread),
        out_shape=jax.ShapeDtypeStruct((part.shape[0] if spread else rows, width), BF16),
        in_specs=[pl.BlockSpec(memory_space=pltpu.VMEM)] * 3,
        out_specs=pl.BlockSpec(memory_space=pltpu.VMEM),
        scratch_shapes=[pltpu.VMEM((n - 1, rows, width), BF16), pltpu.VMEM((n, rows, width), BF16),
                        dma, dma, dma, dma],
        compiler_params=pltpu.CompilerParams(collective_id=cid, has_side_effects=True),
        cost_estimate=pl.CostEstimate(flops=2 * 10**9, bytes_accessed=part.size * 4, transcendentals=0),
        name="settle_spread" if spread else "settle_last",
    )(part, res, gain.reshape(1, -1))


def vmem(count):
    return [pl.BlockSpec(memory_space=pltpu.VMEM)] * count


def carry_ends(tot, mine):
    chunks = tot.shape[1]
    zero = jnp.zeros((1, tot.shape[2]), F32)

    def row(k, s):
        return tot[k, s:s + 1, :]

    fr, fi, br, bi = zero, zero, zero, zero
    pr, pi = zero + 1.0, zero
    for s in range(chunks):
        t = chunks - 1 - s
        nr, ni = cmul(row(4, s), row(5, s), fr, fi)
        fr, fi = nr + row(0, s), ni + row(1, s)
        nr, ni = cmul(row(4, t), row(5, t), br, bi)
        br, bi = nr + row(2, t), ni + row(3, t)
        pr, pi = cmul(row(4, s), row(5, s), pr, pi)
    for k, v in enumerate((fr, fi, br, bi, pr, pi, zero, zero)):
        mine[k:k + 1, :] = v


def carry_starts(tot, got, cin, me, n):
    chunks = tot.shape[1]
    zero = jnp.zeros((1, tot.shape[2]), F32)

    def far(i, carry):
        fr, fi, br, bi = carry
        k = n - 1 - i
        early, late = got.at[k - 1], got.at[n - k - 1]
        nr, ni = cmul(early[4:5, :], early[5:6, :], fr, fi)
        use = me - k >= 0
        fr, fi = jnp.where(use, nr + early[0:1, :], fr), jnp.where(use, ni + early[1:2, :], fi)
        nr, ni = cmul(late[4:5, :], late[5:6, :], br, bi)
        use = me + k < n
        br, bi = jnp.where(use, nr + late[2:3, :], br), jnp.where(use, ni + late[3:4, :], bi)
        return fr, fi, br, bi

    fr, fi, br, bi = lax.fori_loop(0, n - 1, far, (zero, zero, zero, zero))
    for s in range(chunks):
        t = chunks - 1 - s
        cin[0, s:s + 1, :] = fr
        cin[1, s:s + 1, :] = fi
        cin[2, t:t + 1, :] = br
        cin[3, t:t + 1, :] = bi
        nr, ni = cmul(tot[4, s:s + 1, :], tot[5, s:s + 1, :], fr, fi)
        fr, fi = nr + tot[0, s:s + 1, :], ni + tot[1, s:s + 1, :]
        nr, ni = cmul(tot[4, t:t + 1, :], tot[5, t:t + 1, :], br, bi)
        br, bi = nr + tot[2, t:t + 1, :], ni + tot[3, t:t + 1, :]


class Gather:
    def __init__(self, n, sources, targets, parts, pair_first, send, recv, local):
        self.n, self.outer = n, n // 2
        me = lax.axis_index("sp")
        self.me, self.z, self.y = me, me // 2, lax.rem(me, 2)
        self.send, self.recv, self.local = send, recv, local
        self.sources, self.targets = sources, targets
        self.items = []
        for w, src in enumerate(sources):
            rows = src.shape[0] // parts
            for p in range(parts):
                self.items.append((w, pl.ds(p * rows, rows), (w, p) in pair_first))

    def copy(self, i, slot, block, dest, own=False):
        w, rows, _ = self.items[i]
        dst = self.targets[w].at[block, rows]
        src = self.sources[w].at[rows] if own else dst
        return pltpu.make_async_remote_copy(
            src_ref=src, dst_ref=dst, send_sem=self.send.at[i, slot], recv_sem=self.recv.at[i, slot],
            device_id={"sp": dest}, device_id_type=MESH)

    def slot(self, left, r, second):
        return r - 1 + (self.outer - 1) * (int(left) + 2 * int(second))

    def at(self, z, other=False):
        return z * 2 + (1 - self.y if other else self.y)

    def begin(self, first, last):
        o, z = self.outer, self.z
        for i in range(first, last):
            self.copy(i, 4 * (o - 1), self.me, self.at(z, True), own=True).start()

            @pl.when(z + 1 < o)
            def _():
                self.copy(i, self.slot(False, 1, False), self.me, self.at(z + 1), own=True).start()

            @pl.when(z >= 1)
            def _():
                self.copy(i, self.slot(True, 1, False), self.me, self.at(z - 1), own=True).start()

    def begin_local(self):
        for w, src in enumerate(self.sources):
            pltpu.make_async_copy(src, self.targets[w].at[self.me], self.local.at[w]).start()

    def finish(self):
        o, z = self.outer, self.z
        count = len(self.items)
        pair_own = 4 * (o - 1)
        for i in range(count):
            if self.items[i][2]:
                other = self.at(z, True)
                self.copy(i, pair_own, other, other).wait_recv()

                @pl.when(z + 1 < o)
                def _():
                    self.copy(i, self.slot(False, 1, True), other, self.at(z + 1)).start()

                @pl.when(z >= 1)
                def _():
                    self.copy(i, self.slot(True, 1, True), other, self.at(z - 1)).start()

        @pl.loop(1, o)
        def _(r):
            for i in range(count):
                pair_first = self.items[i][2]
                for left in (False, True):
                    far = z + r if left else z - r
                    to = z - 1 if left else z + 1
                    has = far < o if left else far >= 0
                    on = to >= 0 if left else to < o

                    @pl.when(has)
                    def _():
                        self.copy(i, self.slot(left, r, False), self.at(far), self.me).wait_recv()

                        @pl.when(on)
                        def _():
                            self.copy(i, self.slot(left, r + 1, False), self.at(far), self.at(to)).start()

                        if pair_first:
                            self.copy(i, self.slot(left, r, True), self.at(far, True), self.me).wait_recv()

                            @pl.when(on)
                            def _():
                                self.copy(i, self.slot(left, r + 1, True), self.at(far, True), self.at(to)).start()
                        else:
                            self.copy(i, self.slot(left, r, True), self.at(far), self.at(z, True)).start()

        for i in range(count):
            if not self.items[i][2]:
                self.copy(i, pair_own, self.at(z, True), self.me).wait_recv()
            self.copy(i, pair_own, self.me, self.at(z, True), own=True).wait_send()
        for w, src in enumerate(self.sources):
            pltpu.make_async_copy(src, self.targets[w].at[self.me], self.local.at[w]).wait()

        @pl.loop(1, o)
        def _(r):
            for i in range(count):
                pair_first = self.items[i][2]
                for left in (False, True):
                    far = z + r if left else z - r
                    to = z - 1 if left else z + 1
                    sent = z + r - 1 if left else z - r + 1
                    has = far < o if left else far >= 0
                    did = jnp.logical_and(sent < o, to >= 0) if left else jnp.logical_and(sent >= 0, to < o)

                    @pl.when(did)
                    def _():
                        self.copy(i, self.slot(left, r, False), self.at(sent), self.at(to)).wait_send()
                        if pair_first:
                            self.copy(i, self.slot(left, r, True), self.at(sent, True), self.at(to)).wait_send()

                    if not pair_first:
                        @pl.when(has)
                        def _():
                            c = self.copy(i, self.slot(left, r, True), self.at(far, True), self.at(z, True))
                            c.wait_recv()
                            c.wait_send()


def front_kernel(half, width, n, n_tp, parts, pair_first, early,
                 u_ref, pace_ref, rows_ref, in_ref, out_ref, feed_ref, wo_ref, res_ref, gain_ref,
                 gate_ref, value_ref, down_ref,
                 whole_ref, gate_all, value_all, down_all,
                 flow, dec, sf, sb, pf, pb, tot, mine, far, cin, acc, part, got, whole,
                 s0, r0, s1, r1, s2, r2, gsend, grecv, glocal):
    me = lax.axis_index("sp")
    tp = lax.axis_index("tp")
    barrier = pltpu.get_barrier_semaphore()

    @pl.loop(1, n)
    def _(k):
        pl.semaphore_signal(barrier, inc=1, device_id={"sp": lax.rem(me + k, n)}, device_id_type=MESH)

    for k in range(1, n_tp):
        pl.semaphore_signal(barrier, inc=1, device_id={"tp": lax.rem(tp + k, n_tp)}, device_id_type=MESH)
    pl.semaphore_wait(barrier, n - 1 + n_tp - 1)

    weights = Gather(n, (gate_ref, value_ref, down_ref), (gate_all, value_all, down_all), parts, pair_first,
                     gsend, grecv, glocal)
    total = len(weights.items)
    weights.begin(0, early)
    scan_kernel(half, width, u_ref, pace_ref, rows_ref, in_ref, sf, sb, pf, pb, tot, flow, dec)
    carry_ends(tot, mine)

    def shared(k):
        return pltpu.make_async_remote_copy(
            src_ref=mine, dst_ref=far.at[k - 1], send_sem=s0.at[k - 1], recv_sem=r0.at[k - 1],
            device_id={"sp": lax.rem(me + k, n)}, device_id_type=MESH)

    @pl.loop(1, n)
    def _(k):
        shared(k).start()

    weights.begin(early, total)
    weights.begin_local()

    @pl.loop(1, n)
    def _(k):
        shared(k).wait()

    carry_starts(tot, far, cin, me, n)
    readout_kernel(half, width, sf, sb, pf, pb, cin, out_ref, u_ref, feed_ref, wo_ref, part, acc)
    settle_body("tp", n_tp, True, part, res_ref, gain_ref, whole_ref, got, whole, s1, r1, s2, r2)
    weights.finish()


def front(residual, ssm_input, in_map, out_map, damping, log_step, frequency, pacing, feedthrough, w_out,
          gain_mix, w_gate, w_value, w_down):
    positions, chans = ssm_input.shape
    groups, half = damping.shape
    width = chans // groups
    steps = positions // SUB
    flat = groups * half
    model = residual.shape[1]
    n, n_tp = lax.axis_size("sp"), lax.axis_size("tp")
    step = jnp.exp(log_step)[:, None] * jnp.ones((1, half), F32)
    modulus = damping * damping + frequency * frequency
    rows = jnp.stack([step, -damping, frequency, -damping / modulus, -frequency / modulus]).reshape(5, flat)
    u = ssm_input.reshape(SUB, steps, chans).transpose(1, 0, 2).reshape(positions, chans)
    pace = pacing.reshape(SUB, steps).T.reshape(positions, 1) * jnp.ones((1, LANES), F32)
    reps = LANES // half
    in_cols = in_map.reshape(2, chans, 2, half).transpose(0, 2, 1, 3).reshape(4, chans, half)
    in_cols = jnp.tile(in_cols, (1, 1, reps))
    out_rows = out_map.reshape(2, chans, 2, half).transpose(0, 2, 3, 1).reshape(4, half, chans)
    out_rows = jnp.tile(out_rows, (1, reps, 1))
    parts = 2 if n <= 16 else 1
    pair_first = ((2, 0),) if parts == 2 else ()
    items = 3 * parts
    slots = 4 * (n // 2 - 1) + 1
    dma = pltpu.SemaphoreType.DMA
    own = positions // n_tp
    big = pltpu.VMEM((2, positions, flat), F32)
    anywhere = pl.BlockSpec(memory_space=pl.ANY)
    shards_of = (w_gate, w_value, w_down)
    return pl.pallas_call(
        functools.partial(front_kernel, half, width, n, n_tp, parts, pair_first, min(2, items)),
        out_shape=(jax.ShapeDtypeStruct((positions, model), BF16),)
        + tuple(jax.ShapeDtypeStruct((n,) + w.shape, BF16) for w in shards_of),
        in_specs=vmem(9) + [anywhere] * 3,
        out_specs=tuple(vmem(1) + [anywhere] * 3),
        scratch_shapes=[
            pltpu.VMEM((4, positions, LANES), F32), pltpu.VMEM((2, positions, LANES), F32),
            big, big, big, big,
            pltpu.VMEM((6, SUB, flat), F32), pltpu.VMEM((8, flat), F32), pltpu.VMEM((n - 1, 8, flat), F32),
            pltpu.VMEM((4, SUB, flat), F32), pltpu.VMEM((positions, chans), F32),
            pltpu.VMEM((positions, model), BF16),
            pltpu.VMEM((n_tp - 1, own, model), BF16), pltpu.VMEM((n_tp, own, model), BF16),
            dma((n - 1,)), dma((n - 1,)), dma((n_tp - 1,)), dma((n_tp - 1,)), dma((n_tp - 1,)), dma((n_tp - 1,)),
            dma((items, slots)), dma((items, slots)), dma((3,)),
        ],
        compiler_params=pltpu.CompilerParams(collective_id=3, has_side_effects=True),
        cost_estimate=pl.CostEstimate(flops=4 * 10**9, bytes_accessed=10**7, transcendentals=0),
        name="front",
    )(u, pace, rows, in_cols, out_rows, feedthrough.reshape(1, -1), w_out, residual, gain_mix.reshape(1, -1),
      w_gate, w_value, w_down)


def edges(gated):
    n = lax.axis_size("sp")
    before = lax.ppermute(gated[-1:], "sp", [(i, i + 1) for i in range(n - 1)])
    after = lax.ppermute(gated[:1], "sp", [(i + 1, i) for i in range(n - 1)])
    return jnp.concatenate([before, gated, after], axis=0)


def shards(residual, ssm_input, in_map, out_map, damping, log_step, frequency, pacing, feedthrough,
           w_out, gain_mix, w_gate, w_value, conv_taps, w_down, gain_ffn):
    positions = ssm_input.shape[0]
    own_rows = positions // lax.axis_size("tp")
    rows, gate_all, value_all, down_all = front(
        residual, ssm_input, in_map, out_map, damping, log_step, frequency, pacing, feedthrough, w_out,
        gain_mix, w_gate, w_value, w_down)
    gate_all = gate_all.reshape(-1, w_gate.shape[1])
    value_all = value_all.reshape(-1, w_value.shape[1])
    gated = jnp.dot(rows, gate_all, preferred_element_type=F32).astype(BF16)
    padded = edges(gated).astype(F32)
    values = jnp.dot(rows, value_all, preferred_element_type=F32).astype(BF16).astype(F32)
    smoothed = conv_taps[0] * padded[:-2] + conv_taps[1] * padded[1:-1] + conv_taps[2] * padded[2:]
    hidden = (jax.nn.gelu(smoothed) * values).astype(BF16)
    parts = jnp.einsum("th,nhc->tnc", hidden, down_all, preferred_element_type=F32).astype(BF16)
    parts = parts.reshape(positions, -1)
    kept = lax.dynamic_slice_in_dim(rows, lax.axis_index("tp") * own_rows, own_rows, 0)
    return settle(parts, kept, gain_ffn, "tp", False, 5)


def solution(mesh):
    in_specs = (
        P("sp", None), P("sp", "tp"), P(None, "tp", None, None), P(None, "tp", None, None),
        P("tp", None), P("tp"), P("tp", None), P("sp"), P("tp"), P("tp", None), P(),
        P("sp", "tp"), P("sp", "tp"), P(None, "tp"), P("tp", "sp"), P(),
    )
    return jax.shard_map(shards, mesh=mesh, in_specs=in_specs, out_specs=P(("sp", "tp"), None), check_vma=False)
```

```python
import functools
import math

import jax
import jax.numpy as jnp
from jax import lax
from jax.experimental import pallas as pl
from jax.experimental.pallas import tpu as pltpu
from jax.sharding import PartitionSpec as P

deep_alpha = 8.0**0.25
norm_eps = 1e-06
LANES = 128
SUB = 8
MESH = pl.DeviceIdType.MESH
F32 = jnp.float32
BF16 = jnp.bfloat16


def cmul(ar, ai, br, bi):
    return ar * br - ai * bi, ar * bi + ai * br


def sincos(angle):
    turns = jnp.floor(angle * (1.0 / (2.0 * math.pi)) + 0.5)
    rest = (angle - turns * 6.28125) - turns * (2.0 * math.pi - 6.28125)
    half = 0.5 * rest
    sq = half * half
    s = -1.0 / 39916800.0
    for c in (1.0 / 362880.0, -1.0 / 5040.0, 1.0 / 120.0, -1.0 / 6.0, 1.0):
        s = s * sq + c
    s = s * half
    c0 = 1.0 / 479001600.0
    for c in (-1.0 / 3628800.0, 1.0 / 40320.0, -1.0 / 720.0, 1.0 / 24.0, -0.5, 1.0):
        c0 = c0 * sq + c
    return 2.0 * s * c0, 1.0 - 2.0 * s * s


def normalize(pre, gain):
    mean = jnp.mean(pre, axis=-1, keepdims=True)
    cen = pre - mean
    spread = jnp.mean(cen * cen, axis=-1, keepdims=True)
    return cen * lax.rsqrt(spread + norm_eps) * gain


def gelu(x):
    return 0.5 * x * (1.0 + jnp.tanh(0.7978845608028654 * (x + 0.044715 * (x * x * x))))


def tile_ds(tile):
    return pl.ds(pl.multiple_of(tile * LANES, LANES), LANES)


def scan_kernel(half, width, u_ref, pace_ref, rows_ref, in_ref, sf_ref, sb_ref, pf_ref, pb_ref, tot_ref, flow, dec):
    positions = u_ref.shape[0]
    steps = positions // SUB
    tiles = rows_ref.shape[1] // LANES
    per_tile = LANES // half
    chans = u_ref.shape[1]
    row_group = lax.broadcasted_iota(jnp.int32, (chans, LANES), 0) // width
    lane_group = lax.broadcasted_iota(jnp.int32, (chans, LANES), 1) // half

    @pl.loop(0, tiles)
    def _(tile):
        lanes = tile_ds(tile)
        mask = row_group == lane_group + tile * per_tile
        for k in range(4):
            w = jnp.where(mask, in_ref[k].astype(F32), 0.0).astype(BF16)
            flow[k] = jnp.dot(u_ref[...], w, preferred_element_type=F32)
        step = rows_ref[0:1, lanes]
        damp = rows_ref[1:2, lanes]
        freq = rows_ref[2:3, lanes]
        ir = rows_ref[3:4, lanes]
        ii = rows_ref[4:5, lanes]
        one = jnp.ones((SUB, LANES), F32)
        zero = jnp.zeros((SUB, LANES), F32)

        def ahead(j, carry):
            sr, si, pr, pi = carry
            at = pl.ds(pl.multiple_of(j * SUB, SUB), SUB)
            delta = step * pace_ref[at, :]
            mag = jnp.exp(damp * delta)
            sn, cs = sincos(freq * delta)
            dr, di = mag * cs, mag * sn
            fr, fi = cmul(dr - 1.0, di, ir, ii)
            vr, vi = cmul(fr, fi, flow[0, at, :], flow[1, at, :])
            br, bi = cmul(fr, fi, flow[2, at, :], flow[3, at, :])
            flow[2, at, :] = br
            flow[3, at, :] = bi
            dec[0, at, :] = dr
            dec[1, at, :] = di
            sr, si = cmul(dr, di, sr, si)
            sr, si = sr + vr, si + vi
            pr, pi = cmul(dr, di, pr, pi)
            sf_ref[0, at, lanes] = sr
            sf_ref[1, at, lanes] = si
            pf_ref[0, at, lanes] = pr
            pf_ref[1, at, lanes] = pi
            return sr, si, pr, pi

        efr, efi, tr, ti = lax.fori_loop(0, steps, ahead, (zero, zero, one, zero), unroll=4)

        def behind(k, carry):
            sr, si, pr, pi = carry
            at = pl.ds(pl.multiple_of((steps - 1 - k) * SUB, SUB), SUB)
            dr, di = dec[0, at, :], dec[1, at, :]
            sr, si = cmul(dr, di, sr, si)
            sr, si = sr + flow[2, at, :], si + flow[3, at, :]
            pr, pi = cmul(dr, di, pr, pi)
            sb_ref[0, at, lanes] = sr
            sb_ref[1, at, lanes] = si
            pb_ref[0, at, lanes] = pr
            pb_ref[1, at, lanes] = pi
            return sr, si, pr, pi

        ebr, ebi, _, _ = lax.fori_loop(0, steps, behind, (zero, zero, one, zero), unroll=4)
        for k, v in enumerate((efr, efi, ebr, ebi, tr, ti)):
            tot_ref[k, :, lanes] = v


def readout_kernel(half, width, sf_ref, sb_ref, pf_ref, pb_ref, cin_ref, out_ref, u_ref, feed_ref, wo_ref, mixed_ref, acc):
    positions = u_ref.shape[0]
    steps = positions // SUB
    tiles = cin_ref.shape[2] // LANES
    per_tile = LANES // half
    chans = u_ref.shape[1]
    col_group = lax.broadcasted_iota(jnp.int32, (LANES, chans), 1) // width
    row_group = lax.broadcasted_iota(jnp.int32, (LANES, chans), 0) // half
    acc[...] = feed_ref[...] * u_ref[...].astype(F32)

    @pl.loop(0, tiles)
    def _(tile):
        lanes = tile_ds(tile)
        mask = col_group == row_group + tile * per_tile
        total = acc[...]
        for d, (s_ref, p_ref) in enumerate(((sf_ref, pf_ref), (sb_ref, pb_ref))):
            cr = jnp.broadcast_to(cin_ref[2 * d, :, lanes][None], (steps, SUB, LANES)).reshape(positions, LANES)
            ci = jnp.broadcast_to(cin_ref[2 * d + 1, :, lanes][None], (steps, SUB, LANES)).reshape(positions, LANES)
            ar, ai = cmul(p_ref[0, :, lanes], p_ref[1, :, lanes], cr, ci)
            for k, st in enumerate((ar + s_ref[0, :, lanes], ai + s_ref[1, :, lanes])):
                w = jnp.where(mask, out_ref[2 * d + k].astype(F32), 0.0).astype(BF16)
                total += jnp.dot(st.astype(BF16), w, preferred_element_type=F32)
        acc[...] = total

    channels = gelu(acc[...]).astype(BF16)
    row = lax.broadcasted_iota(jnp.int32, (positions, positions), 0)
    col = lax.broadcasted_iota(jnp.int32, (positions, positions), 1)
    pick = jnp.where(col == lax.rem(row, steps) * SUB + row // steps, 1.0, 0.0).astype(BF16)
    channels = jnp.dot(pick, channels, preferred_element_type=F32).astype(BF16)
    cols = wo_ref.shape[1]
    piece = min(512, cols)
    for c in range(cols // piece):
        at = slice(c * piece, (c + 1) * piece)
        mixed_ref[:, at] = jnp.dot(channels, wo_ref[:, at], preferred_element_type=F32).astype(BF16)


def vmem(count):
    return [pl.BlockSpec(memory_space=pltpu.VMEM)] * count


def carry_ends(tot, mine):
    chunks = tot.shape[1]
    zero = jnp.zeros((1, tot.shape[2]), F32)

    def row(k, s):
        return tot[k, s:s + 1, :]

    fr, fi, br, bi = zero, zero, zero, zero
    pr, pi = zero + 1.0, zero
    for s in range(chunks):
        t = chunks - 1 - s
        nr, ni = cmul(row(4, s), row(5, s), fr, fi)
        fr, fi = nr + row(0, s), ni + row(1, s)
        nr, ni = cmul(row(4, t), row(5, t), br, bi)
        br, bi = nr + row(2, t), ni + row(3, t)
        pr, pi = cmul(row(4, s), row(5, s), pr, pi)
    for k, v in enumerate((fr, fi, br, bi, pr, pi, zero, zero)):
        mine[k:k + 1, :] = v


def carry_starts(tot, got, cin, me, n):
    chunks = tot.shape[1]
    zero = jnp.zeros((1, tot.shape[2]), F32)

    def far(i, carry):
        fr, fi, br, bi = carry
        k = n - 1 - i
        early, late = got.at[k - 1], got.at[n - k - 1]
        nr, ni = cmul(early[4:5, :], early[5:6, :], fr, fi)
        use = me - k >= 0
        fr, fi = jnp.where(use, nr + early[0:1, :], fr), jnp.where(use, ni + early[1:2, :], fi)
        nr, ni = cmul(late[4:5, :], late[5:6, :], br, bi)
        use = me + k < n
        br, bi = jnp.where(use, nr + late[2:3, :], br), jnp.where(use, ni + late[3:4, :], bi)
        return fr, fi, br, bi

    fr, fi, br, bi = lax.fori_loop(0, n - 1, far, (zero, zero, zero, zero))
    for s in range(chunks):
        t = chunks - 1 - s
        cin[0, s:s + 1, :] = fr
        cin[1, s:s + 1, :] = fi
        cin[2, t:t + 1, :] = br
        cin[3, t:t + 1, :] = bi
        nr, ni = cmul(tot[4, s:s + 1, :], tot[5, s:s + 1, :], fr, fi)
        fr, fi = nr + tot[0, s:s + 1, :], ni + tot[1, s:s + 1, :]
        nr, ni = cmul(tot[4, t:t + 1, :], tot[5, t:t + 1, :], br, bi)
        br, bi = nr + tot[2, t:t + 1, :], ni + tot[3, t:t + 1, :]


class Gather:
    def __init__(self, n, half_of, sources, targets, pair_first, send, recv, local, csend, crecv):
        self.n, self.m, self.outer = n, n // 2, n // 4
        me = lax.axis_index("sp")
        self.me, self.side = me, me // self.m
        place = lax.rem(me, self.m)
        self.z, self.y = place // 2, lax.rem(place, 2)
        self.mate = lax.rem(me + self.m, n)
        self.send, self.recv, self.local, self.csend, self.crecv = send, recv, local, csend, crecv
        self.sources, self.targets, self.half_of = sources, targets, half_of
        self.items = [(w, kind) for kind in range(2) for w in range(len(sources))]
        self.pair_first = pair_first

    def cut(self, w, side):
        dim, size = self.half_of[w]
        start = pl.multiple_of(side * (self.sources[w].shape[dim] - size), LANES)
        at = pl.ds(start, size)
        return self.sources[w].at[at] if dim == 0 else self.sources[w].at[:, at]

    def device(self, z, other=False):
        return self.side * self.m + z * 2 + (1 - self.y if other else self.y)

    def block(self, i, z, other=False):
        side = 1 - self.side if self.items[i][1] else self.side
        return side * self.m + z * 2 + (1 - self.y if other else self.y)

    def copy(self, i, slot, block, dest, own=False):
        w, kind = self.items[i]
        dst = self.targets[w].at[block]
        src = self.cut(w, self.side) if own and kind == 0 else dst
        return pltpu.make_async_remote_copy(
            src_ref=src, dst_ref=dst, send_sem=self.send.at[i, slot], recv_sem=self.recv.at[i, slot],
            device_id={"sp": dest}, device_id_type=MESH)

    def cross(self, w, block):
        return pltpu.make_async_remote_copy(
            src_ref=self.cut(w, 1 - self.side), dst_ref=self.targets[w].at[block], send_sem=self.csend.at[w],
            recv_sem=self.crecv.at[w], device_id={"sp": self.mate}, device_id_type=MESH)

    def slot(self, left, r, second):
        return r - 1 + (self.outer - 1) * (int(left) + 2 * int(second))

    @property
    def pair_own(self):
        return 4 * (self.outer - 1)

    def begin(self, i):
        o, z = self.outer, self.z
        mine = self.block(i, z)
        self.copy(i, self.pair_own, mine, self.device(z, True), own=True).start()

        @pl.when(z + 1 < o)
        def _():
            self.copy(i, self.slot(False, 1, False), mine, self.device(z + 1), own=True).start()

        @pl.when(z >= 1)
        def _():
            self.copy(i, self.slot(True, 1, False), mine, self.device(z - 1), own=True).start()

    def begin_local(self):
        for w in range(len(self.sources)):
            pltpu.make_async_copy(self.cut(w, self.side), self.targets[w].at[self.me], self.local.at[w]).start()

    def second(self, i):
        o, z = self.outer, self.z
        other = self.block(i, z, True)
        self.copy(i, self.pair_own, other, self.me).wait_recv()

        @pl.when(z + 1 < o)
        def _():
            self.copy(i, self.slot(False, 1, True), other, self.device(z + 1)).start()

        @pl.when(z >= 1)
        def _():
            self.copy(i, self.slot(True, 1, True), other, self.device(z - 1)).start()

    def pump(self, which):
        o, z = self.outer, self.z

        @pl.loop(1, o)
        def _(r):
            for i in which:
                pair_first = i in self.pair_first
                for left in (False, True):
                    far = z + r if left else z - r
                    to = z - 1 if left else z + 1
                    has = far < o if left else far >= 0
                    on = to >= 0 if left else to < o

                    @pl.when(has)
                    def _():
                        self.copy(i, self.slot(left, r, False), self.block(i, far), self.me).wait_recv()

                        @pl.when(on)
                        def _():
                            self.copy(i, self.slot(left, r + 1, False), self.block(i, far), self.device(to)).start()

                        if pair_first:
                            self.copy(i, self.slot(left, r, True), self.block(i, far, True), self.me).wait_recv()

                            @pl.when(on)
                            def _():
                                self.copy(i, self.slot(left, r + 1, True), self.block(i, far, True),
                                          self.device(to)).start()
                        else:
                            self.copy(i, self.slot(left, r, True), self.block(i, far), self.device(z, True)).start()

    def finish(self):
        o, z = self.outer, self.z
        count = len(self.items)
        for i in range(count):
            if i not in self.pair_first:
                self.copy(i, self.pair_own, self.block(i, z, True), self.me).wait_recv()
            self.copy(i, self.pair_own, self.block(i, z), self.device(z, True), own=True).wait_send()
        for w in range(len(self.sources)):
            pltpu.make_async_copy(self.cut(w, self.side), self.targets[w].at[self.me], self.local.at[w]).wait()
            self.cross(w, self.me).wait_send()

        @pl.loop(1, o)
        def _(r):
            for i in range(count):
                pair_first = i in self.pair_first
                for left in (False, True):
                    far = z + r if left else z - r
                    to = z - 1 if left else z + 1
                    sent = z + r - 1 if left else z - r + 1
                    has = far < o if left else far >= 0
                    did = jnp.logical_and(sent < o, to >= 0) if left else jnp.logical_and(sent >= 0, to < o)

                    @pl.when(did)
                    def _():
                        self.copy(i, self.slot(left, r, False), self.block(i, sent), self.device(to)).wait_send()
                        if pair_first:
                            self.copy(i, self.slot(left, r, True), self.block(i, sent, True),
                                      self.device(to)).wait_send()

                    if not pair_first:
                        @pl.when(has)
                        def _():
                            c = self.copy(i, self.slot(left, r, True), self.block(i, far, True), self.device(z, True))
                            c.wait_recv()
                            c.wait_send()


def to_peers(axis, n, src, slots, send, recv):
    me = lax.axis_index(axis)
    copies = []
    for k in range(1, n):
        c = pltpu.make_async_remote_copy(
            src_ref=src(lax.rem(me + k, n)), dst_ref=slots(k), send_sem=send.at[k - 1], recv_sem=recv.at[k - 1],
            device_id={axis: lax.rem(me + k, n)}, device_id_type=MESH)
        c.start()
        copies.append(c)
    return copies


def span(who, rows, base=0):
    return pl.ds(pl.multiple_of(base + who * rows, rows), rows)


def mix_rows(n, mate, side, part, res_ref, gain_ref, rows_ref, got, whole, theirs, s1, r1, s2, r2, s3, r3, sm, rm):
    me = lax.axis_index("tp")
    positions = part.shape[0]
    rows = positions // n
    copies = to_peers("tp", n, lambda peer: part.at[span(peer, rows)], lambda k: got.at[k - 1], s1, r1)
    total = part[span(me, rows), :].astype(F32) + deep_alpha * res_ref[span(me, rows), :].astype(F32)
    for k in range(1, n):
        copies[k - 1].wait()
        total = total + got[k - 1].astype(F32)
    result = normalize(total, gain_ref[...]).astype(BF16)
    whole[0] = result
    swap = pltpu.make_async_remote_copy(
        src_ref=whole.at[0], dst_ref=theirs.at[0], send_sem=sm.at[0], recv_sem=rm.at[0],
        device_id={"sp": mate}, device_id_type=MESH)
    swap.start()
    first = to_peers("tp", n, lambda peer: whole.at[0], lambda k: whole.at[k], s2, r2)
    mine, other = side * positions, (1 - side) * positions
    rows_ref[span(me, rows, mine), :] = result
    swap.wait()
    later = to_peers("tp", n, lambda peer: theirs.at[0], lambda k: theirs.at[k], s3, r3)
    rows_ref[span(me, rows, other), :] = theirs[0]
    for k in range(1, n):
        first[k - 1].wait()
        rows_ref[span(lax.rem(me + n - k, n), rows, mine), :] = whole[k]
    return later, lambda k: rows_ref.at[span(lax.rem(me + n - k, n), rows, other)]


def last_kernel(n, n_sp, part_ref, res_ref, gain_ref, out_ref, got_a, got_b, away, home, s1, r1, s2, r2, sm, rm):
    me = lax.axis_index("tp")
    sp = lax.axis_index("sp")
    m = n_sp // 2
    side, mate = sp // m, lax.rem(sp + m, n_sp)
    rows = res_ref.shape[0]
    positions = rows * n
    barrier = pltpu.get_barrier_semaphore()
    for k in range(1, n):
        pl.semaphore_signal(barrier, inc=1, device_id={"tp": lax.rem(me + k, n)}, device_id_type=MESH)
    pl.semaphore_signal(barrier, inc=1, device_id={"sp": mate}, device_id_type=MESH)
    pl.semaphore_wait(barrier, n)
    mine, other = side * positions, (1 - side) * positions
    out_first = to_peers("tp", n, lambda p: part_ref.at[span(p, rows, other)], lambda k: got_a.at[k - 1], s1, r1)
    in_later = to_peers("tp", n, lambda p: part_ref.at[span(p, rows, mine)], lambda k: got_b.at[k - 1], s2, r2)
    total = part_ref[span(me, rows, other), :].astype(F32)
    for k in range(1, n):
        out_first[k - 1].wait()
        total = total + got_a[k - 1].astype(F32)
    away[...] = total.astype(BF16)
    swap = pltpu.make_async_remote_copy(
        src_ref=away, dst_ref=home, send_sem=sm.at[0], recv_sem=rm.at[0], device_id={"sp": mate}, device_id_type=MESH)
    swap.start()
    total = part_ref[span(me, rows, mine), :].astype(F32) + deep_alpha * res_ref[...].astype(F32)
    for k in range(1, n):
        in_later[k - 1].wait()
        total = total + got_b[k - 1].astype(F32)
    swap.wait()
    out_ref[...] = normalize(total + home[...].astype(F32), gain_ref[...]).astype(BF16)


def last(part, res, gain):
    n, n_sp = lax.axis_size("tp"), lax.axis_size("sp")
    rows, width = res.shape
    dma = pltpu.SemaphoreType.DMA
    return pl.pallas_call(
        functools.partial(last_kernel, n, n_sp),
        out_shape=jax.ShapeDtypeStruct((rows, width), BF16),
        in_specs=vmem(3),
        out_specs=pl.BlockSpec(memory_space=pltpu.VMEM),
        scratch_shapes=[pltpu.VMEM((n - 1, rows, width), BF16), pltpu.VMEM((n - 1, rows, width), BF16),
                        pltpu.VMEM((rows, width), BF16), pltpu.VMEM((rows, width), BF16),
                        dma((n - 1,)), dma((n - 1,)), dma((n - 1,)), dma((n - 1,)), dma((1,)), dma((1,))],
        compiler_params=pltpu.CompilerParams(collective_id=5, has_side_effects=True),
        name="last_sum",
    )(part, res, gain.reshape(1, -1))


def front_kernel(half, width, n, n_tp, half_of, pair_first, early,
                 u_ref, pace_ref, rows_ref, in_ref, out_ref, feed_ref, wo_ref, res_ref, gain_ref,
                 gate_ref, value_ref, down_ref,
                 whole_ref, gate_all, value_all, down_all,
                 flow, dec, sf, sb, pf, pb, tot, mine, far, cin, acc, part, got, whole, theirs,
                 s0, r0, s1, r1, s2, r2, s3, r3, sm, rm, gsend, grecv, glocal, csend, crecv):
    me = lax.axis_index("sp")
    tp = lax.axis_index("tp")
    barrier = pltpu.get_barrier_semaphore()

    @pl.loop(1, n)
    def _(k):
        pl.semaphore_signal(barrier, inc=1, device_id={"sp": lax.rem(me + k, n)}, device_id_type=MESH)

    for k in range(1, n_tp):
        pl.semaphore_signal(barrier, inc=1, device_id={"tp": lax.rem(tp + k, n_tp)}, device_id_type=MESH)
    pl.semaphore_wait(barrier, n - 1 + n_tp - 1)

    weights = Gather(n, half_of, (gate_ref, value_ref, down_ref), (gate_all, value_all, down_all), pair_first,
                     gsend, grecv, glocal, csend, crecv)
    count = len(half_of)
    for i in range(early):
        weights.begin(i)
    scan_kernel(half, width, u_ref, pace_ref, rows_ref, in_ref, sf, sb, pf, pb, tot, flow, dec)
    carry_ends(tot, mine)

    def shared(k):
        return pltpu.make_async_remote_copy(
            src_ref=mine, dst_ref=far.at[k - 1], send_sem=s0.at[k - 1], recv_sem=r0.at[k - 1],
            device_id={"sp": lax.rem(me + k, n)}, device_id_type=MESH)

    @pl.loop(1, n)
    def _(k):
        shared(k).start()

    for i in range(early, count):
        weights.begin(i)
    for w in range(count):
        weights.cross(w, me).start()
    weights.begin_local()

    @pl.loop(1, n)
    def _(k):
        shared(k).wait()

    carry_starts(tot, far, cin, me, n)
    readout_kernel(half, width, sf, sb, pf, pb, cin, out_ref, u_ref, feed_ref, wo_ref, part, acc)
    for i in pair_first:
        weights.second(i)
    weights.pump([i for i in range(count) if i not in pair_first])
    later, place = mix_rows(n_tp, weights.mate, weights.side, part, res_ref, gain_ref, whole_ref, got, whole, theirs,
                            s1, r1, s2, r2, s3, r3, sm, rm)
    for w in range(count):
        weights.cross(w, weights.mate).wait_recv()
        weights.begin(count + w)
    for k in range(1, n_tp):
        later[k - 1].wait()
        place(k)[...] = theirs[k]
    weights.pump(list(pair_first))
    weights.pump([count + w for w in range(count)])
    weights.finish()


def front(residual, ssm_input, in_map, out_map, damping, log_step, frequency, pacing, feedthrough, w_out,
          gain_mix, w_gate, w_value, w_down):
    positions, chans = ssm_input.shape
    groups, half = damping.shape
    width = chans // groups
    steps = positions // SUB
    flat = groups * half
    model = residual.shape[1]
    n, n_tp = lax.axis_size("sp"), lax.axis_size("tp")
    step = jnp.exp(log_step)[:, None] * jnp.ones((1, half), F32)
    modulus = damping * damping + frequency * frequency
    rows = jnp.stack([step, -damping, frequency, -damping / modulus, -frequency / modulus]).reshape(5, flat)
    u = ssm_input.reshape(SUB, steps, chans).transpose(1, 0, 2).reshape(positions, chans)
    pace = pacing.reshape(SUB, steps).T.reshape(positions, 1) * jnp.ones((1, LANES), F32)
    reps = LANES // half
    in_cols = in_map.reshape(2, chans, 2, half).transpose(0, 2, 1, 3).reshape(4, chans, half)
    in_cols = jnp.tile(in_cols, (1, 1, reps))
    out_rows = out_map.reshape(2, chans, 2, half).transpose(0, 2, 3, 1).reshape(4, half, chans)
    out_rows = jnp.tile(out_rows, (1, reps, 1))
    hidden = w_gate.shape[1]
    share = -(-hidden // (2 * LANES)) * LANES
    half_of = ((1, share), (1, share), (0, share))
    pair_first = (0,)
    items = 6
    slots = 4 * (n // 4 - 1) + 1
    dma = pltpu.SemaphoreType.DMA
    own = positions // n_tp
    big = pltpu.VMEM((2, positions, flat), F32)
    anywhere = pl.BlockSpec(memory_space=pl.ANY)
    shards_of = (w_gate, w_value, w_down)
    return pl.pallas_call(
        functools.partial(front_kernel, half, width, n, n_tp, half_of, pair_first, 2),
        out_shape=(jax.ShapeDtypeStruct((2 * positions, model), BF16),)
        + tuple(jax.ShapeDtypeStruct(
            (n,) + tuple(size if d == dim else c for d, c in enumerate(w.shape)), BF16)
            for w, (dim, size) in zip(shards_of, half_of)),
        in_specs=vmem(9) + [anywhere] * 3,
        out_specs=tuple(vmem(1) + [anywhere] * 3),
        scratch_shapes=[
            pltpu.VMEM((4, positions, LANES), F32), pltpu.VMEM((2, positions, LANES), F32),
            big, big, big, big,
            pltpu.VMEM((6, SUB, flat), F32), pltpu.VMEM((8, flat), F32), pltpu.VMEM((n - 1, 8, flat), F32),
            pltpu.VMEM((4, SUB, flat), F32), pltpu.VMEM((positions, chans), F32),
            pltpu.VMEM((positions, model), BF16),
            pltpu.VMEM((n_tp - 1, own, model), BF16), pltpu.VMEM((n_tp, own, model), BF16),
            pltpu.VMEM((n_tp, own, model), BF16),
            dma((n - 1,)), dma((n - 1,)), dma((n_tp - 1,)), dma((n_tp - 1,)), dma((n_tp - 1,)), dma((n_tp - 1,)),
            dma((n_tp - 1,)), dma((n_tp - 1,)), dma((1,)), dma((1,)),
            dma((items, slots)), dma((items, slots)), dma((3,)), dma((3,)), dma((3,)),
        ],
        compiler_params=pltpu.CompilerParams(collective_id=3, has_side_effects=True),
        cost_estimate=pl.CostEstimate(flops=4 * 10**9, bytes_accessed=10**7, transcendentals=0),
        name="front",
    )(u, pace, rows, in_cols, out_rows, feedthrough.reshape(1, -1), w_out, residual, gain_mix.reshape(1, -1),
      w_gate, w_value, w_down)


def edges(gated):
    n = lax.axis_size("sp")
    m = n // 2
    place = lax.rem(lax.axis_index("sp"), m)
    ring = [(s * m + b, s * m + (b + 1) % m) for s in range(2) for b in range(m)]
    before = lax.ppermute(gated[:, -1:], "sp", ring)
    after = lax.ppermute(gated[:, :1], "sp", [(j, i) for i, j in ring])
    zero = jnp.zeros_like(before[:1])
    before = jnp.where(place == 0, jnp.concatenate([zero, before[:1]]), before)
    after = jnp.where(place == m - 1, jnp.concatenate([after[1:], zero]), after)
    return jnp.concatenate([before, gated, after], axis=1)


def shards(residual, ssm_input, in_map, out_map, damping, log_step, frequency, pacing, feedthrough,
           w_out, gain_mix, w_gate, w_value, conv_taps, w_down, gain_ffn):
    positions = ssm_input.shape[0]
    own_rows = positions // lax.axis_size("tp")
    rows, gate_all, value_all, down_all = front(
        residual, ssm_input, in_map, out_map, damping, log_step, frequency, pacing, feedthrough, w_out,
        gain_mix, w_gate, w_value, w_down)
    model = residual.shape[1]
    m = lax.axis_size("sp") // 2
    side = lax.axis_index("sp") // m
    share = gate_all.shape[2]
    start = side * (conv_taps.shape[1] - share)
    overlap = 2 * share - conv_taps.shape[1]
    taps = lax.dynamic_slice_in_dim(conv_taps, start, share, 1)
    gated = jnp.dot(rows, gate_all.reshape(model, share), preferred_element_type=F32).astype(BF16)
    padded = edges(gated.reshape(2, positions, share)).astype(F32)
    values = jnp.dot(rows, value_all.reshape(model, share), preferred_element_type=F32).astype(BF16)
    values = values.reshape(2, positions, share).astype(F32)
    smoothed = taps[0] * padded[:, :-2] + taps[1] * padded[:, 1:-1] + taps[2] * padded[:, 2:]
    hidden = jax.nn.gelu(smoothed) * values
    unit = lax.broadcasted_iota(jnp.int32, (1, 1, share), 2)
    hidden = jnp.where(jnp.logical_and(side == 1, unit < overlap), 0.0, hidden).astype(BF16)
    hidden = hidden.reshape(2 * positions, share)
    parts = jnp.einsum("th,nhc->tnc", hidden, down_all, preferred_element_type=F32).astype(BF16)
    parts = parts.reshape(2 * positions, model)
    kept = lax.dynamic_slice_in_dim(rows, side * positions + lax.axis_index("tp") * own_rows, own_rows, 0)
    return last(parts, kept, gain_ffn)


def solution(mesh):
    in_specs = (
        P("sp", None), P("sp", "tp"), P(None, "tp", None, None), P(None, "tp", None, None),
        P("tp", None), P("tp"), P("tp", None), P("sp"), P("tp"), P("tp", None), P(),
        P("sp", "tp"), P("sp", "tp"), P(None, "tp"), P("tp", "sp"), P(),
    )
    return jax.shard_map(shards, mesh=mesh, in_specs=in_specs, out_specs=P(("sp", "tp"), None), check_vma=False)
```

```python
import functools
import math

import jax
import jax.numpy as jnp
from jax import lax
from jax.experimental import pallas as pl
from jax.experimental.pallas import tpu as pltpu
from jax.sharding import PartitionSpec as P

deep_alpha = 8.0**0.25
norm_eps = 1e-06
LANES = 128
SUB = 8
MESH = pl.DeviceIdType.MESH
F32 = jnp.float32
BF16 = jnp.bfloat16


def cmul(ar, ai, br, bi):
    return ar * br - ai * bi, ar * bi + ai * br


def sincos(angle):
    turns = jnp.floor(angle * (1.0 / (2.0 * math.pi)) + 0.5)
    rest = (angle - turns * 6.28125) - turns * (2.0 * math.pi - 6.28125)
    half = 0.5 * rest
    sq = half * half
    s = -1.0 / 39916800.0
    for c in (1.0 / 362880.0, -1.0 / 5040.0, 1.0 / 120.0, -1.0 / 6.0, 1.0):
        s = s * sq + c
    s = s * half
    c0 = 1.0 / 479001600.0
    for c in (-1.0 / 3628800.0, 1.0 / 40320.0, -1.0 / 720.0, 1.0 / 24.0, -0.5, 1.0):
        c0 = c0 * sq + c
    return 2.0 * s * c0, 1.0 - 2.0 * s * s


def normalize(pre, gain):
    mean = jnp.mean(pre, axis=-1, keepdims=True)
    cen = pre - mean
    spread = jnp.mean(cen * cen, axis=-1, keepdims=True)
    return cen * lax.rsqrt(spread + norm_eps) * gain


def gelu(x):
    return 0.5 * x * (1.0 + jnp.tanh(0.7978845608028654 * (x + 0.044715 * (x * x * x))))


def tile_ds(tile):
    return pl.ds(pl.multiple_of(tile * LANES, LANES), LANES)


def scan_kernel(half, width, u_ref, pace_ref, rows_ref, in_ref, sf_ref, sb_ref, pf_ref, pb_ref, tot_ref, flow, dec):
    positions = u_ref.shape[0]
    steps = positions // SUB
    tiles = rows_ref.shape[1] // LANES
    per_tile = LANES // half
    chans = u_ref.shape[1]
    row_group = lax.broadcasted_iota(jnp.int32, (chans, LANES), 0) // width
    lane_group = lax.broadcasted_iota(jnp.int32, (chans, LANES), 1) // half

    @pl.loop(0, tiles)
    def _(tile):
        lanes = tile_ds(tile)
        mask = row_group == lane_group + tile * per_tile
        for k in range(4):
            w = jnp.where(mask, in_ref[k].astype(F32), 0.0).astype(BF16)
            flow[k] = jnp.dot(u_ref[...], w, preferred_element_type=F32)
        step = rows_ref[0:1, lanes]
        damp = rows_ref[1:2, lanes]
        freq = rows_ref[2:3, lanes]
        ir = rows_ref[3:4, lanes]
        ii = rows_ref[4:5, lanes]
        one = jnp.ones((SUB, LANES), F32)
        zero = jnp.zeros((SUB, LANES), F32)

        def ahead(j, carry):
            sr, si, pr, pi = carry
            at = pl.ds(pl.multiple_of(j * SUB, SUB), SUB)
            delta = step * pace_ref[at, :]
            mag = jnp.exp(damp * delta)
            sn, cs = sincos(freq * delta)
            dr, di = mag * cs, mag * sn
            fr, fi = cmul(dr - 1.0, di, ir, ii)
            vr, vi = cmul(fr, fi, flow[0, at, :], flow[1, at, :])
            br, bi = cmul(fr, fi, flow[2, at, :], flow[3, at, :])
            flow[2, at, :] = br
            flow[3, at, :] = bi
            dec[0, at, :] = dr
            dec[1, at, :] = di
            sr, si = cmul(dr, di, sr, si)
            sr, si = sr + vr, si + vi
            pr, pi = cmul(dr, di, pr, pi)
            sf_ref[0, at, lanes] = sr
            sf_ref[1, at, lanes] = si
            pf_ref[0, at, lanes] = pr
            pf_ref[1, at, lanes] = pi
            return sr, si, pr, pi

        efr, efi, tr, ti = lax.fori_loop(0, steps, ahead, (zero, zero, one, zero), unroll=4)

        def behind(k, carry):
            sr, si, pr, pi = carry
            at = pl.ds(pl.multiple_of((steps - 1 - k) * SUB, SUB), SUB)
            dr, di = dec[0, at, :], dec[1, at, :]
            sr, si = cmul(dr, di, sr, si)
            sr, si = sr + flow[2, at, :], si + flow[3, at, :]
            pr, pi = cmul(dr, di, pr, pi)
            sb_ref[0, at, lanes] = sr
            sb_ref[1, at, lanes] = si
            pb_ref[0, at, lanes] = pr
            pb_ref[1, at, lanes] = pi
            return sr, si, pr, pi

        ebr, ebi, _, _ = lax.fori_loop(0, steps, behind, (zero, zero, one, zero), unroll=4)
        for k, v in enumerate((efr, efi, ebr, ebi, tr, ti)):
            tot_ref[k, :, lanes] = v


def readout_kernel(half, width, sf_ref, sb_ref, pf_ref, pb_ref, cin_ref, out_ref, u_ref, feed_ref, wo_ref, mixed_ref, acc):
    positions = u_ref.shape[0]
    steps = positions // SUB
    tiles = cin_ref.shape[2] // LANES
    per_tile = LANES // half
    chans = u_ref.shape[1]
    col_group = lax.broadcasted_iota(jnp.int32, (LANES, chans), 1) // width
    row_group = lax.broadcasted_iota(jnp.int32, (LANES, chans), 0) // half
    acc[...] = feed_ref[...] * u_ref[...].astype(F32)

    @pl.loop(0, tiles)
    def _(tile):
        lanes = tile_ds(tile)
        mask = col_group == row_group + tile * per_tile
        total = acc[...]
        for d, (s_ref, p_ref) in enumerate(((sf_ref, pf_ref), (sb_ref, pb_ref))):
            cr = jnp.broadcast_to(cin_ref[2 * d, :, lanes][None], (steps, SUB, LANES)).reshape(positions, LANES)
            ci = jnp.broadcast_to(cin_ref[2 * d + 1, :, lanes][None], (steps, SUB, LANES)).reshape(positions, LANES)
            ar, ai = cmul(p_ref[0, :, lanes], p_ref[1, :, lanes], cr, ci)
            for k, st in enumerate((ar + s_ref[0, :, lanes], ai + s_ref[1, :, lanes])):
                w = jnp.where(mask, out_ref[2 * d + k].astype(F32), 0.0).astype(BF16)
                total += jnp.dot(st.astype(BF16), w, preferred_element_type=F32)
        acc[...] = total

    channels = gelu(acc[...]).astype(BF16)
    row = lax.broadcasted_iota(jnp.int32, (positions, positions), 0)
    col = lax.broadcasted_iota(jnp.int32, (positions, positions), 1)
    pick = jnp.where(col == lax.rem(row, steps) * SUB + row // steps, 1.0, 0.0).astype(BF16)
    channels = jnp.dot(pick, channels, preferred_element_type=F32).astype(BF16)
    cols = wo_ref.shape[1]
    piece = min(512, cols)
    for c in range(cols // piece):
        at = slice(c * piece, (c + 1) * piece)
        mixed_ref[:, at] = jnp.dot(channels, wo_ref[:, at], preferred_element_type=F32).astype(BF16)


def vmem(count):
    return [pl.BlockSpec(memory_space=pltpu.VMEM)] * count


def carry_ends(tot, mine):
    chunks = tot.shape[1]
    zero = jnp.zeros((1, tot.shape[2]), F32)

    def row(k, s):
        return tot[k, s:s + 1, :]

    fr, fi, br, bi = zero, zero, zero, zero
    pr, pi = zero + 1.0, zero
    for s in range(chunks):
        t = chunks - 1 - s
        nr, ni = cmul(row(4, s), row(5, s), fr, fi)
        fr, fi = nr + row(0, s), ni + row(1, s)
        nr, ni = cmul(row(4, t), row(5, t), br, bi)
        br, bi = nr + row(2, t), ni + row(3, t)
        pr, pi = cmul(row(4, s), row(5, s), pr, pi)
    for k, v in enumerate((fr, fi, br, bi, pr, pi, zero, zero)):
        mine[k:k + 1, :] = v


def carry_starts(tot, got, cin, me, n):
    chunks = tot.shape[1]
    zero = jnp.zeros((1, tot.shape[2]), F32)

    def far(i, carry):
        fr, fi, br, bi = carry
        k = n - 1 - i
        early, late = got.at[k - 1], got.at[n - k - 1]
        nr, ni = cmul(early[4:5, :], early[5:6, :], fr, fi)
        use = me - k >= 0
        fr, fi = jnp.where(use, nr + early[0:1, :], fr), jnp.where(use, ni + early[1:2, :], fi)
        nr, ni = cmul(late[4:5, :], late[5:6, :], br, bi)
        use = me + k < n
        br, bi = jnp.where(use, nr + late[2:3, :], br), jnp.where(use, ni + late[3:4, :], bi)
        return fr, fi, br, bi

    fr, fi, br, bi = lax.fori_loop(0, n - 1, far, (zero, zero, zero, zero))
    for s in range(chunks):
        t = chunks - 1 - s
        cin[0, s:s + 1, :] = fr
        cin[1, s:s + 1, :] = fi
        cin[2, t:t + 1, :] = br
        cin[3, t:t + 1, :] = bi
        nr, ni = cmul(tot[4, s:s + 1, :], tot[5, s:s + 1, :], fr, fi)
        fr, fi = nr + tot[0, s:s + 1, :], ni + tot[1, s:s + 1, :]
        nr, ni = cmul(tot[4, t:t + 1, :], tot[5, t:t + 1, :], br, bi)
        br, bi = nr + tot[2, t:t + 1, :], ni + tot[3, t:t + 1, :]


class Gather:
    def __init__(self, n, half_of, sources, targets, pair_first, send, recv, local, csend, crecv):
        self.n, self.m, self.outer = n, n // 2, n // 4
        me = lax.axis_index("sp")
        self.me, self.side = me, me // self.m
        place = lax.rem(me, self.m)
        self.z, self.y = place // 2, lax.rem(place, 2)
        self.mate = lax.rem(me + self.m, n)
        self.send, self.recv, self.local, self.csend, self.crecv = send, recv, local, csend, crecv
        self.sources, self.targets, self.half_of = sources, targets, half_of
        self.items = [(w, kind) for kind in range(2) for w in range(len(sources))]
        self.pair_first = pair_first

    def cut(self, w, side):
        dim, size = self.half_of[w]
        start = pl.multiple_of(side * (self.sources[w].shape[dim] - size), LANES)
        at = pl.ds(start, size)
        return self.sources[w].at[at] if dim == 0 else self.sources[w].at[:, at]

    def device(self, z, other=False):
        return self.side * self.m + z * 2 + (1 - self.y if other else self.y)

    def block(self, i, z, other=False):
        side = 1 - self.side if self.items[i][1] else self.side
        return side * self.m + z * 2 + (1 - self.y if other else self.y)

    def copy(self, i, slot, block, dest, own=False):
        w, kind = self.items[i]
        dst = self.targets[w].at[block]
        src = self.cut(w, self.side) if own and kind == 0 else dst
        return pltpu.make_async_remote_copy(
            src_ref=src, dst_ref=dst, send_sem=self.send.at[i, slot], recv_sem=self.recv.at[i, slot],
            device_id={"sp": dest}, device_id_type=MESH)

    def cross(self, w, block):
        return pltpu.make_async_remote_copy(
            src_ref=self.cut(w, 1 - self.side), dst_ref=self.targets[w].at[block], send_sem=self.csend.at[w],
            recv_sem=self.crecv.at[w], device_id={"sp": self.mate}, device_id_type=MESH)

    def slot(self, left, r, second):
        return r - 1 + (self.outer - 1) * (int(left) + 2 * int(second))

    @property
    def pair_own(self):
        return 4 * (self.outer - 1)

    def begin(self, i):
        o, z = self.outer, self.z
        mine = self.block(i, z)
        self.copy(i, self.pair_own, mine, self.device(z, True), own=True).start()

        @pl.when(z + 1 < o)
        def _():
            self.copy(i, self.slot(False, 1, False), mine, self.device(z + 1), own=True).start()

        @pl.when(z >= 1)
        def _():
            self.copy(i, self.slot(True, 1, False), mine, self.device(z - 1), own=True).start()

    def begin_local(self):
        for w in range(len(self.sources)):
            pltpu.make_async_copy(self.cut(w, self.side), self.targets[w].at[self.me], self.local.at[w]).start()

    def second(self, i):
        o, z = self.outer, self.z
        other = self.block(i, z, True)
        self.copy(i, self.pair_own, other, self.me).wait_recv()

        @pl.when(z + 1 < o)
        def _():
            self.copy(i, self.slot(False, 1, True), other, self.device(z + 1)).start()

        @pl.when(z >= 1)
        def _():
            self.copy(i, self.slot(True, 1, True), other, self.device(z - 1)).start()

    def pump(self, which):
        o, z = self.outer, self.z

        @pl.loop(1, o)
        def _(r):
            for i in which:
                pair_first = i in self.pair_first
                for left in (False, True):
                    far = z + r if left else z - r
                    to = z - 1 if left else z + 1
                    has = far < o if left else far >= 0
                    on = to >= 0 if left else to < o

                    @pl.when(has)
                    def _():
                        self.copy(i, self.slot(left, r, False), self.block(i, far), self.me).wait_recv()

                        @pl.when(on)
                        def _():
                            self.copy(i, self.slot(left, r + 1, False), self.block(i, far), self.device(to)).start()

                        if pair_first:
                            self.copy(i, self.slot(left, r, True), self.block(i, far, True), self.me).wait_recv()

                            @pl.when(on)
                            def _():
                                self.copy(i, self.slot(left, r + 1, True), self.block(i, far, True),
                                          self.device(to)).start()
                        else:
                            self.copy(i, self.slot(left, r, True), self.block(i, far), self.device(z, True)).start()

    def finish(self):
        o, z = self.outer, self.z
        count = len(self.items)
        for i in range(count):
            if i not in self.pair_first:
                self.copy(i, self.pair_own, self.block(i, z, True), self.me).wait_recv()
            self.copy(i, self.pair_own, self.block(i, z), self.device(z, True), own=True).wait_send()
        for w in range(len(self.sources)):
            pltpu.make_async_copy(self.cut(w, self.side), self.targets[w].at[self.me], self.local.at[w]).wait()
            self.cross(w, self.me).wait_send()

        @pl.loop(1, o)
        def _(r):
            for i in range(count):
                pair_first = i in self.pair_first
                for left in (False, True):
                    far = z + r if left else z - r
                    to = z - 1 if left else z + 1
                    sent = z + r - 1 if left else z - r + 1
                    has = far < o if left else far >= 0
                    did = jnp.logical_and(sent < o, to >= 0) if left else jnp.logical_and(sent >= 0, to < o)

                    @pl.when(did)
                    def _():
                        self.copy(i, self.slot(left, r, False), self.block(i, sent), self.device(to)).wait_send()
                        if pair_first:
                            self.copy(i, self.slot(left, r, True), self.block(i, sent, True),
                                      self.device(to)).wait_send()

                    if not pair_first:
                        @pl.when(has)
                        def _():
                            c = self.copy(i, self.slot(left, r, True), self.block(i, far, True), self.device(z, True))
                            c.wait_recv()
                            c.wait_send()


def to_peers(axis, n, src, slots, send, recv):
    me = lax.axis_index(axis)
    copies = []
    for k in range(1, n):
        c = pltpu.make_async_remote_copy(
            src_ref=src(lax.rem(me + k, n)), dst_ref=slots(k), send_sem=send.at[k - 1], recv_sem=recv.at[k - 1],
            device_id={axis: lax.rem(me + k, n)}, device_id_type=MESH)
        c.start()
        copies.append(c)
    return copies


def span(who, rows, base=0):
    return pl.ds(pl.multiple_of(base + who * rows, rows), rows)


def mix_rows(n, mate, side, part, res_ref, gain_ref, rows_ref, got, whole, theirs, s1, r1, s2, r2, s3, r3, sm, rm,
             pass_on):
    me = lax.axis_index("tp")
    positions = part.shape[0]
    rows = positions // n
    copies = to_peers("tp", n, lambda peer: part.at[span(peer, rows)], lambda k: got.at[k - 1], s1, r1)
    total = part[span(me, rows), :].astype(F32) + deep_alpha * res_ref[span(me, rows), :].astype(F32)
    for k in range(1, n):
        copies[k - 1].wait()
        total = total + got[k - 1].astype(F32)
    result = normalize(total, gain_ref[...]).astype(BF16)
    whole[0] = result
    swap = pltpu.make_async_remote_copy(
        src_ref=whole.at[0], dst_ref=theirs.at[0], send_sem=sm.at[0], recv_sem=rm.at[0],
        device_id={"sp": mate}, device_id_type=MESH)
    swap.start()
    first = to_peers("tp", n, lambda peer: whole.at[0], lambda k: whole.at[k], s2, r2)
    mine, other = side * positions, (1 - side) * positions
    rows_ref[span(me, rows, mine), :] = result
    pass_on()
    swap.wait()
    later = to_peers("tp", n, lambda peer: theirs.at[0], lambda k: theirs.at[k], s3, r3)
    rows_ref[span(me, rows, other), :] = theirs[0]
    for k in range(1, n):
        first[k - 1].wait()
        rows_ref[span(lax.rem(me + n - k, n), rows, mine), :] = whole[k]
    return later, lambda k: rows_ref.at[span(lax.rem(me + n - k, n), rows, other)]


def last_kernel(n, n_sp, part_ref, res_ref, gain_ref, out_ref, pair_got, stage, got, away, home,
                s1, r1, s2, r2, sm, rm):
    me = lax.axis_index("tp")
    sp = lax.axis_index("sp")
    m = n_sp // 2
    side, mate = sp // m, lax.rem(sp + m, n_sp)
    outer, parity = me // 2, lax.rem(me, 2)
    pairs = n // 2
    partner = outer * 2 + 1 - parity
    rows = res_ref.shape[0]
    positions = rows * n
    barrier = pltpu.get_barrier_semaphore()

    def at(k):
        return lax.rem(outer + k, pairs) * 2

    pl.semaphore_signal(barrier, inc=1, device_id={"tp": partner}, device_id_type=MESH)
    for k in range(1, pairs):
        pl.semaphore_signal(barrier, inc=1, device_id={"tp": at(k) + parity}, device_id_type=MESH)
    pl.semaphore_signal(barrier, inc=1, device_id={"sp": mate}, device_id_type=MESH)
    pl.semaphore_wait(barrier, 1 + pairs)
    bases = ((1 - side) * positions, side * positions)
    near, far, kept = {}, {}, []
    order = list(range(1, pairs)) + [0]
    for b, base in enumerate(bases):
        for k in order:
            near[b, k] = pltpu.make_async_remote_copy(
                src_ref=part_ref.at[span(at(k) + 1 - parity, rows, base)], dst_ref=pair_got.at[b, k],
                send_sem=s1.at[b, k], recv_sem=r1.at[b, k], device_id={"tp": partner}, device_id_type=MESH)
            near[b, k].start()
    for b, base in enumerate(bases):
        for k in order:
            near[b, k].wait()
            both = part_ref[span(at(k) + parity, rows, base), :].astype(F32) + pair_got[b, k].astype(F32)
            if k == 0:
                kept.append(both)
                continue
            stage[b, k] = both.astype(BF16)
            far[b, k] = pltpu.make_async_remote_copy(
                src_ref=stage.at[b, k], dst_ref=got.at[b, k], send_sem=s2.at[b, k], recv_sem=r2.at[b, k],
                device_id={"tp": at(k) + parity}, device_id_type=MESH)
            far[b, k].start()
    total = kept[0]
    for k in range(1, pairs):
        far[0, k].wait()
        total = total + got[0, k].astype(F32)
    away[...] = total.astype(BF16)
    swap = pltpu.make_async_remote_copy(
        src_ref=away, dst_ref=home, send_sem=sm.at[0], recv_sem=rm.at[0], device_id={"sp": mate}, device_id_type=MESH)
    swap.start()
    total = kept[1] + deep_alpha * res_ref[...].astype(F32)
    for k in range(1, pairs):
        far[1, k].wait()
        total = total + got[1, k].astype(F32)
    swap.wait()
    out_ref[...] = normalize(total + home[...].astype(F32), gain_ref[...]).astype(BF16)


def last(part, res, gain):
    n, n_sp = lax.axis_size("tp"), lax.axis_size("sp")
    rows, width = res.shape
    dma = pltpu.SemaphoreType.DMA((2, n // 2))
    one = pltpu.SemaphoreType.DMA((1,))
    quads = pltpu.VMEM((2, n // 2, rows, width), BF16)
    row = pltpu.VMEM((rows, width), BF16)
    return pl.pallas_call(
        functools.partial(last_kernel, n, n_sp),
        out_shape=jax.ShapeDtypeStruct((rows, width), BF16),
        in_specs=vmem(3),
        out_specs=pl.BlockSpec(memory_space=pltpu.VMEM),
        scratch_shapes=[quads, quads, quads, row, row, dma, dma, dma, dma, one, one],
        compiler_params=pltpu.CompilerParams(collective_id=5, has_side_effects=True),
        name="last_sum",
    )(part, res, gain.reshape(1, -1))


def front_kernel(half, width, n, n_tp, half_of, pair_first, early,
                 u_ref, pace_ref, rows_ref, in_ref, out_ref, feed_ref, wo_ref, res_ref, gain_ref,
                 gate_ref, value_ref, down_ref,
                 whole_ref, gate_all, value_all, down_all,
                 flow, dec, sf, sb, pf, pb, tot, mine, far, cin, acc, part, got, whole, theirs,
                 s0, r0, s1, r1, s2, r2, s3, r3, sm, rm, gsend, grecv, glocal, csend, crecv):
    me = lax.axis_index("sp")
    tp = lax.axis_index("tp")
    barrier = pltpu.get_barrier_semaphore()

    @pl.loop(1, n)
    def _(k):
        pl.semaphore_signal(barrier, inc=1, device_id={"sp": lax.rem(me + k, n)}, device_id_type=MESH)

    for k in range(1, n_tp):
        pl.semaphore_signal(barrier, inc=1, device_id={"tp": lax.rem(tp + k, n_tp)}, device_id_type=MESH)
    pl.semaphore_wait(barrier, n - 1 + n_tp - 1)

    weights = Gather(n, half_of, (gate_ref, value_ref, down_ref), (gate_all, value_all, down_all), pair_first,
                     gsend, grecv, glocal, csend, crecv)
    count = len(half_of)
    for i in range(early):
        weights.begin(i)
    scan_kernel(half, width, u_ref, pace_ref, rows_ref, in_ref, sf, sb, pf, pb, tot, flow, dec)
    carry_ends(tot, mine)

    def shared(k):
        return pltpu.make_async_remote_copy(
            src_ref=mine, dst_ref=far.at[k - 1], send_sem=s0.at[k - 1], recv_sem=r0.at[k - 1],
            device_id={"sp": lax.rem(me + k, n)}, device_id_type=MESH)

    @pl.loop(1, n)
    def _(k):
        shared(k).start()

    for w in range(early):
        weights.cross(w, me).start()
    for i in range(early, count):
        weights.begin(i)
        weights.cross(i, me).start()
    weights.begin_local()

    @pl.loop(1, n)
    def _(k):
        shared(k).wait()

    carry_starts(tot, far, cin, me, n)
    readout_kernel(half, width, sf, sb, pf, pb, cin, out_ref, u_ref, feed_ref, wo_ref, part, acc)
    for i in pair_first:
        weights.second(i)
    weights.pump([i for i in range(count) if i not in pair_first])

    def pass_on():
        for w in range(count):
            weights.cross(w, weights.mate).wait_recv()
            weights.begin(count + w)

    later, place = mix_rows(n_tp, weights.mate, weights.side, part, res_ref, gain_ref, whole_ref, got, whole, theirs,
                            s1, r1, s2, r2, s3, r3, sm, rm, pass_on)
    for k in range(1, n_tp):
        later[k - 1].wait()
        place(k)[...] = theirs[k]
    weights.pump(list(pair_first))
    weights.pump([count + w for w in range(count)])
    weights.finish()


def front(residual, ssm_input, in_map, out_map, damping, log_step, frequency, pacing, feedthrough, w_out,
          gain_mix, w_gate, w_value, w_down):
    positions, chans = ssm_input.shape
    groups, half = damping.shape
    width = chans // groups
    steps = positions // SUB
    flat = groups * half
    model = residual.shape[1]
    n, n_tp = lax.axis_size("sp"), lax.axis_size("tp")
    step = jnp.exp(log_step)[:, None] * jnp.ones((1, half), F32)
    modulus = damping * damping + frequency * frequency
    rows = jnp.stack([step, -damping, frequency, -damping / modulus, -frequency / modulus]).reshape(5, flat)
    u = ssm_input.reshape(SUB, steps, chans).transpose(1, 0, 2).reshape(positions, chans)
    pace = pacing.reshape(SUB, steps).T.reshape(positions, 1) * jnp.ones((1, LANES), F32)
    reps = LANES // half
    in_cols = in_map.reshape(2, chans, 2, half).transpose(0, 2, 1, 3).reshape(4, chans, half)
    in_cols = jnp.tile(in_cols, (1, 1, reps))
    out_rows = out_map.reshape(2, chans, 2, half).transpose(0, 2, 3, 1).reshape(4, half, chans)
    out_rows = jnp.tile(out_rows, (1, reps, 1))
    hidden = w_gate.shape[1]
    share = -(-hidden // (2 * LANES)) * LANES
    half_of = ((1, share), (1, share), (0, share))
    pair_first = (0,)
    items = 6
    slots = 4 * (n // 4 - 1) + 1
    dma = pltpu.SemaphoreType.DMA
    own = positions // n_tp
    big = pltpu.VMEM((2, positions, flat), F32)
    anywhere = pl.BlockSpec(memory_space=pl.ANY)
    shards_of = (w_gate, w_value, w_down)
    return pl.pallas_call(
        functools.partial(front_kernel, half, width, n, n_tp, half_of, pair_first, 2),
        out_shape=(jax.ShapeDtypeStruct((2 * positions, model), BF16),)
        + tuple(jax.ShapeDtypeStruct(
            (n,) + tuple(size if d == dim else c for d, c in enumerate(w.shape)), BF16)
            for w, (dim, size) in zip(shards_of, half_of)),
        in_specs=vmem(9) + [anywhere] * 3,
        out_specs=tuple(vmem(1) + [anywhere] * 3),
        scratch_shapes=[
            pltpu.VMEM((4, positions, LANES), F32), pltpu.VMEM((2, positions, LANES), F32),
            big, big, big, big,
            pltpu.VMEM((6, SUB, flat), F32), pltpu.VMEM((8, flat), F32), pltpu.VMEM((n - 1, 8, flat), F32),
            pltpu.VMEM((4, SUB, flat), F32), pltpu.VMEM((positions, chans), F32),
            pltpu.VMEM((positions, model), BF16),
            pltpu.VMEM((n_tp - 1, own, model), BF16), pltpu.VMEM((n_tp, own, model), BF16),
            pltpu.VMEM((n_tp, own, model), BF16),
            dma((n - 1,)), dma((n - 1,)), dma((n_tp - 1,)), dma((n_tp - 1,)), dma((n_tp - 1,)), dma((n_tp - 1,)),
            dma((n_tp - 1,)), dma((n_tp - 1,)), dma((1,)), dma((1,)),
            dma((items, slots)), dma((items, slots)), dma((3,)), dma((3,)), dma((3,)),
        ],
        compiler_params=pltpu.CompilerParams(collective_id=3, has_side_effects=True),
        cost_estimate=pl.CostEstimate(flops=4 * 10**9, bytes_accessed=10**7, transcendentals=0),
        name="front",
    )(u, pace, rows, in_cols, out_rows, feedthrough.reshape(1, -1), w_out, residual, gain_mix.reshape(1, -1),
      w_gate, w_value, w_down)


def edges(gated):
    n = lax.axis_size("sp")
    m = n // 2
    place = lax.rem(lax.axis_index("sp"), m)
    ring = [(s * m + b, s * m + (b + 1) % m) for s in range(2) for b in range(m)]
    before = lax.ppermute(gated[:, -1:], "sp", ring)
    after = lax.ppermute(gated[:, :1], "sp", [(j, i) for i, j in ring])
    zero = jnp.zeros_like(before[:1])
    before = jnp.where(place == 0, jnp.concatenate([zero, before[:1]]), before)
    after = jnp.where(place == m - 1, jnp.concatenate([after[1:], zero]), after)
    return jnp.concatenate([before, gated, after], axis=1)


def shards(residual, ssm_input, in_map, out_map, damping, log_step, frequency, pacing, feedthrough,
           w_out, gain_mix, w_gate, w_value, conv_taps, w_down, gain_ffn):
    positions = ssm_input.shape[0]
    own_rows = positions // lax.axis_size("tp")
    rows, gate_all, value_all, down_all = front(
        residual, ssm_input, in_map, out_map, damping, log_step, frequency, pacing, feedthrough, w_out,
        gain_mix, w_gate, w_value, w_down)
    model = residual.shape[1]
    m = lax.axis_size("sp") // 2
    side = lax.axis_index("sp") // m
    share = gate_all.shape[2]
    start = side * (conv_taps.shape[1] - share)
    overlap = 2 * share - conv_taps.shape[1]
    taps = lax.dynamic_slice_in_dim(conv_taps, start, share, 1)
    gated = jnp.dot(rows, gate_all.reshape(model, share), preferred_element_type=F32).astype(BF16)
    padded = edges(gated.reshape(2, positions, share)).astype(F32)
    values = jnp.dot(rows, value_all.reshape(model, share), preferred_element_type=F32).astype(BF16)
    values = values.reshape(2, positions, share).astype(F32)
    smoothed = taps[0] * padded[:, :-2] + taps[1] * padded[:, 1:-1] + taps[2] * padded[:, 2:]
    hidden = jax.nn.gelu(smoothed) * values
    unit = lax.broadcasted_iota(jnp.int32, (1, 1, share), 2)
    hidden = jnp.where(jnp.logical_and(side == 1, unit < overlap), 0.0, hidden).astype(BF16)
    hidden = hidden.reshape(2 * positions, share)
    parts = jnp.einsum("th,nhc->tnc", hidden, down_all, preferred_element_type=F32).astype(BF16)
    parts = parts.reshape(2 * positions, model)
    kept = lax.dynamic_slice_in_dim(rows, side * positions + lax.axis_index("tp") * own_rows, own_rows, 0)
    return last(parts, kept, gain_ffn)


def solution(mesh):
    in_specs = (
        P("sp", None), P("sp", "tp"), P(None, "tp", None, None), P(None, "tp", None, None),
        P("tp", None), P("tp"), P("tp", None), P("sp"), P("tp"), P("tp", None), P(),
        P("sp", "tp"), P("sp", "tp"), P(None, "tp"), P("tp", "sp"), P(),
    )
    return jax.shard_map(shards, mesh=mesh, in_specs=in_specs, out_specs=P(("sp", "tp"), None), check_vma=False)
```
